32 devices in a mesh: sp: 16 (over z, y, x), tp: 2 (over core).
Axes of the slice: x: 2, y: 2, z: 4, core: 2. Of those that a mesh axis runs over, the one named last changes fastest.
Arguments:
- queries: bfloat16 [2048, 768], P('sp', 'tp'), may hold values from -6 to 6
- latents: bfloat16 [2048, 512], P('sp'), may hold values from -6 to 6
- rot_key: bfloat16 [2048, 32], P('sp'), may hold values from -6 to 6
- kv_weight: bfloat16 [512, 1024], P(None, 'tp'), may hold values from -0.25 to 0.25
- log_sums: float32 [2048, 8], P('sp', 'tp'), may hold values from 4 to 14, as said below
- outputs: bfloat16 [2048, 512], P('sp', 'tp'), may hold values from -4 to 4
- out_grad: bfloat16 [2048, 512], P('sp', 'tp'), may hold values from -96 to 96
Outputs:
- query_grad: bfloat16 [2048, 768], P('sp', 'tp')
- key_grad: bfloat16 [2048, 512], P('sp', 'tp')
- value_grad: bfloat16 [2048, 512], P('sp', 'tp')
- rot_grad: float32 [2048, 32], P('sp')
- weight_grad: float32 [512, 1024], P('sp', 'tp')
The draws below stay inside these ranges and needn't reach their ends.
Inputs may be any that keep to these rules, and one draw needn't show every extreme that they name: `log_sums`: each value lies within one half of log(2048) + 0.5.
All inputs are finite; a program needn't handle non-finite values.
Results may differ from the reference program's by a relative error of at most 0.004.
The reference program's roundings to bfloat16 on the way (of `joined`, `key_full`, `probs_b` and `dscore`) count: a program that leaves them out, or rounds other values in their place, can miss the bound.
Values may be sent and summed in bfloat16 or wider, within the bound.
A program may use at most 64 MiB of HBM per device.

```python
import math
import jax
import jax.numpy as jnp
from jax import lax

HEADS = 8
RANK = 512
NOPE_DIM = 64
ROPE_DIM = 32
VALUE_DIM = 64
SEQ = 2048


def draw_log_sums(key, part):
    center = math.log(SEQ) + 0.5
    return center + jax.random.uniform(key, (SEQ, HEADS), jnp.float32, -0.5, 0.5)


def with_spikes(result, own_key, source, target, parts, factor):
    def block_of(dim):
        return (jnp.arange(result.shape[dim]) // (result.shape[dim] // parts)).reshape((-1,) + (1,) * (result.ndim - 1 - dim))

    near = jax.random.permutation(own_key, parts)[block_of(target)]
    other_side = (block_of(target) + parts // 2) % parts
    return jnp.where((block_of(source) == near) | (block_of(source) == other_side), factor * result, result)


def block_scale(rng, dims, split, low, top_value):
    def one(dim, blocks):
        draws = jax.random.uniform(jax.random.fold_in(jax.random.fold_in(rng, 6), dim), (blocks,), jnp.float32, low / len(split), top_value / len(split))
        return jnp.repeat(jnp.exp(draws), dims[dim] // blocks).reshape((-1,) + (1,) * (len(dims) - dim - 1))

    loudness = one(*split[0])
    for cut in split[1:]:
        loudness = loudness * one(*cut)
    return loudness


def normal_values(key, shape, deviation, reach, shards=(), kind=jnp.bfloat16):
    array = jax.random.normal(key, shape, jnp.float32) * deviation
    if len(shards) > 0:
        array = block_scale(key, shape, shards, -0.22, 0.18) * array
    return jnp.clip(array, min=-reach, max=reach).astype(kind)


def noise_with(own_key, extent, spread, limit, pieces, heavy, held_as=jnp.bfloat16):
    entries = spread * jax.random.normal(own_key, extent, jnp.float32)
    if pieces:
        entries = entries * block_scale(own_key, extent, pieces, -0.22, 0.18)
    return jnp.clip(with_spikes(entries, jax.random.fold_in(own_key, 3), *heavy), -limit, limit).astype(held_as)


def setup_inputs(seed: int = 0) -> dict:
    splits = jax.random.split(jax.random.key(seed), 8)
    queries = normal_values(splits[0], (SEQ, HEADS * (NOPE_DIM + ROPE_DIM)), 1.0, 6.0, ((0, 16), (1, 2)))
    latents = normal_values(splits[1], (SEQ, RANK), 1.0, 6.0, ((0, 16),))
    rot_key = normal_values(splits[2], (SEQ, ROPE_DIM), 1.0, 6.0, ((0, 16),))
    kv_weight = normal_values(splits[3], (RANK, HEADS * (NOPE_DIM + VALUE_DIM)), RANK ** -0.5, 0.25, ((1, 2),))
    log_sums = draw_log_sums(jax.random.fold_in(splits[7], 71), 0)
    outputs = normal_values(splits[5], (SEQ, HEADS * VALUE_DIM), 0.3, 4.0, ((0, 16), (1, 2)))
    out_grad = noise_with(splits[6], (SEQ, HEADS * VALUE_DIM), (SEQ ** 0.5 / 4), 96.0, ((0, 16), (1, 2)), (0, 1, 16, 2.0))
    return dict(queries=queries, latents=latents, rot_key=rot_key, kv_weight=kv_weight, log_sums=log_sums, outputs=outputs, out_grad=out_grad)


def round_keep(values):
    rounded = values.astype(jnp.bfloat16)
    rounded = lax.optimization_barrier(rounded)
    return rounded.astype(jnp.float32)


def reference(queries, latents, rot_key, kv_weight, log_sums, outputs, out_grad):
    head_dim = NOPE_DIM + ROPE_DIM
    score_scale = head_dim ** -0.5
    joined = jnp.dot(latents, kv_weight, preferred_element_type=jnp.float32).astype(jnp.bfloat16)
    joined = joined.reshape(SEQ, HEADS, NOPE_DIM + VALUE_DIM).astype(jnp.float32)
    rotary = jnp.broadcast_to(rot_key.astype(jnp.float32)[:, None, :], (SEQ, HEADS, ROPE_DIM))
    key_full = jnp.concatenate([joined[:, :, :NOPE_DIM], rotary], axis=-1)
    values = joined[:, :, NOPE_DIM:]
    query_full = queries.astype(jnp.float32).reshape(SEQ, HEADS, head_dim)
    grad_full = out_grad.astype(jnp.float32).reshape(SEQ, HEADS, VALUE_DIM)
    row_delta = jnp.sum(outputs.astype(jnp.float32).reshape(SEQ, HEADS, VALUE_DIM) * grad_full, axis=-1)
    block_rows = math.gcd(SEQ, 512)
    block_count = SEQ // block_rows

    def block_step(totals, block_index):
        key_total, value_total = totals
        begin_row = (block_index * block_rows).astype(jnp.int32)
        query_block = lax.dynamic_slice_in_dim(query_full, begin_row, block_rows, 0)
        grad_block = lax.dynamic_slice_in_dim(grad_full, begin_row, block_rows, 0)
        log_block = lax.dynamic_slice_in_dim(log_sums, begin_row, block_rows, 0)
        delta_block = lax.dynamic_slice_in_dim(row_delta, begin_row, block_rows, 0)
        scores = jnp.einsum('qhd,khd->hqk', query_block, key_full) * score_scale
        probs = jnp.exp(scores - log_block.T[:, :, None])
        dprob = jnp.einsum('qhd,khd->hqk', grad_block, values)
        dscore = round_keep(probs * (dprob - delta_block.T[:, :, None]))
        probs_b = round_keep(probs)
        query_part = (jnp.einsum('hqk,khd->qhd', dscore, key_full) * score_scale).astype(jnp.bfloat16)
        key_total = key_total + jnp.einsum('hqk,qhd->khd', dscore, query_block) * score_scale
        value_total = value_total + jnp.einsum('hqk,qhd->khd', probs_b, grad_block)
        return (key_total, value_total), query_part

    start_totals = (jnp.zeros((SEQ, HEADS, head_dim), jnp.float32), jnp.zeros((SEQ, HEADS, VALUE_DIM), jnp.float32))
    (key_total, value_total), query_blocks = lax.scan(block_step, start_totals, jnp.arange(block_count, dtype=jnp.int32))
    query_grad = query_blocks.reshape(SEQ, HEADS * head_dim)
    rot_grad = jnp.sum(key_total[:, :, NOPE_DIM:], axis=1)
    key_grad = key_total[:, :, :NOPE_DIM].astype(jnp.bfloat16)
    value_grad = value_total.astype(jnp.bfloat16)
    stacked = jnp.concatenate([key_grad, value_grad], axis=-1).reshape(SEQ, HEADS * (NOPE_DIM + VALUE_DIM))
    weight_grad = jnp.dot(latents.T, stacked, preferred_element_type=jnp.float32)
    return (query_grad, key_grad.reshape(SEQ, HEADS * NOPE_DIM), value_grad.reshape(SEQ, HEADS * VALUE_DIM), rot_grad, weight_grad)
```

```python
import functools
import math

import jax
import jax.numpy as jnp
from jax import lax
from jax.experimental import pallas as pl
from jax.experimental.pallas import tpu as pltpu
from jax.sharding import PartitionSpec as P

NOPE = 64
ROPE = 32
VDIM = 64
HEAD = NOPE + ROPE
LANES = 128
STATS = 8
VMEM_BYTES = 67043328
SPARE = 8192
MESH = pl.DeviceIdType.MESH
F32 = jnp.float32
BF16 = jnp.bfloat16
KV_PART = BF16
DQ_PART = F32
WG_PART = BF16


def dot(x, y, dims):
    return lax.dot_general(x, y, (dims, ((), ())), preferred_element_type=F32)


def three_terms(x):
    hi = x.astype(BF16)
    rest = x - hi.astype(F32)
    mid = rest.astype(BF16)
    low = (rest - mid.astype(F32)).astype(BF16)
    return hi, mid, low


def repeat(start, stop, body):
    if stop - start <= 4:
        for i in range(start, stop):
            body(i)
    else:
        def step(i, carry):
            body(i)
            return carry

        lax.fori_loop(start, stop, step, 0)


def add_all(terms):
    return functools.reduce(lambda x, y: x + y, terms)


def power_of_two(n):
    return n & (n - 1) == 0


def partner(n, i, d, sign):
    if not power_of_two(n):
        return lax.rem(i + sign * d + n, n)
    bit = 1
    result = i
    while bit <= d:
        if d & bit:
            result = result + bit * (1 - 2 * lax.rem(i // bit, 2))
        bit *= 2
    return result


def distances(n):
    if not power_of_two(n):
        return list(range(1, n))
    return list(range(n // 2, n)) + list(range(1, n // 2))


def kernel(
    S, TP, H, GY, GX,
    q_in, lat_in, rot_in, w_in, log_in, out_in, go_in,
    qg_ref, kg_ref, vg_ref, rg_ref, wg_ref,
    q_ref, lat_ref, rot_ref, w_ref, log_ref, out_ref, go_ref, loads,
    qs, pk, wq, kb, lb, rp, dqa, dqs, dqr, kvs, kvr, own_kv, own_rot,
    kvo, kvh, ro, rr, rt, wgs, wgr, dqo, dqh,
    s1q, r1q, s1k, r1k, s1l, r1l, s2q, r2q, s2k, r2k, s3q, r3q, s3k, r3k,
    s4q, r4q, s4k, r4k, s4r, r4r, s5, r5, s6, r6, s8, r8,
):
    G = GY * GX
    T = q_ref.shape[0]
    me = lax.axis_index("sp")
    tpi = lax.axis_index("tp")
    a, b = me // G, lax.rem(me, G)
    y, x = b // GX, lax.rem(b, GX)
    scale = HEAD ** (-0.5)
    log2e = math.log2(math.e)
    far = distances(H)
    quarter = T * ROPE // LANES

    barrier = pltpu.get_barrier_semaphore()

    def greet(to):
        pl.semaphore_signal(barrier, inc=1, device_id={"sp": to}, device_id_type=MESH)

    def greet_tp(i):
        pl.semaphore_signal(barrier, inc=1, device_id={"tp": lax.rem(tpi + i, TP)}, device_id_type=MESH)

    def at_z(z):
        return z * G + b

    def at_y(e):
        return a * G + lax.rem(y + e, GY) * GX + x

    def at_x(e):
        return a * G + y * GX + lax.rem(x + e, GX)

    pairs = (
        (q_in, q_ref), (go_in, go_ref), (out_in, out_ref), (log_in, log_ref),
        (lat_in, lat_ref), (w_in, w_ref), (rot_in, rot_ref),
    )
    fetch = [pltpu.make_async_copy(u, v, loads.at[i]) for i, (u, v) in enumerate(pairs)]
    for f in fetch:
        f.start()
    for d in far:
        greet(at_z(partner(H, a, d, 1)))
    repeat(1, GY, lambda e: greet(at_y(e)))
    repeat(1, GX, lambda e: greet(at_x(e)))
    repeat(1, TP, greet_tp)

    def copy(src, dst, ssem, rsem, sp):
        return pltpu.make_async_remote_copy(
            src_ref=src, dst_ref=dst, send_sem=ssem, recv_sem=rsem,
            device_id={"sp": sp}, device_id_type=MESH,
        )

    def copy_tp(src, dst, ssem, rsem, i):
        return pltpu.make_async_remote_copy(
            src_ref=src, dst_ref=dst, send_sem=ssem, recv_sem=rsem,
            device_id={"tp": lax.rem(tpi + i, TP)}, device_id_type=MESH,
        )

    for f in fetch[:4]:
        f.wait()
    prod = out_ref[...].astype(F32) * go_ref[...].astype(F32)
    high = prod.astype(BF16)
    rest = (prod - high.astype(F32)).astype(BF16)
    head_of = lax.broadcasted_iota(jnp.int32, (8 * -(-H // 8), H * VDIM), 1) // VDIM
    picks = (head_of == lax.broadcasted_iota(jnp.int32, head_of.shape, 0)).astype(F32).astype(BF16)
    deltas = dot(picks, high, ((1,), (1,))) + dot(picks, rest, ((1,), (1,)))
    logs = log_ref[...] * log2e
    for j in range(H):
        start = HEAD * j
        qs[j, :T, :] = jnp.concatenate(
            [q_ref[:, start : start + NOPE], go_ref[:, VDIM * j : VDIM * (j + 1)]], axis=1)
        turned = q_ref[:, start + NOPE : start + HEAD]
        qs[j, T : T + quarter, :] = jnp.concatenate(
            [turned[quarter * i : quarter * (i + 1)] for i in range(LANES // ROPE)], axis=1)
        terms = three_terms(logs[j : j + 1]) + three_terms(deltas[j : j + 1])
        qs[j, T + quarter :, :] = jnp.concatenate(
            [t.astype(F32) for t in terms] + [jnp.zeros((STATS - 6, T), F32)], axis=0).astype(BF16)
    wq[y, a] = qs[a]
    pl.semaphore_wait(barrier, H - 1 + GY - 1 + GX - 1 + TP - 1)

    def first_q(d):
        to = partner(H, a, d, 1)
        return copy(qs.at[to], wq.at[y, a], s1q.at[d - 1], r1q.at[d - 1], at_z(to))

    def first_k(d):
        to = partner(H, a, d, 1)
        return copy(pk.at[to], kb.at[x, a], s1k.at[d - 1], r1k.at[d - 1], at_z(to))

    def relay_q(d, e):
        src = wq.at[y, partner(H, a, d, -1)]
        return copy(src, src, s2q.at[e - 1, d], r2q.at[e - 1, d], at_y(e))

    def relay_k(d, e):
        src = kb.at[x, partner(H, a, d, -1)]
        return copy(src, src, s2k.at[e - 1, d], r2k.at[e - 1, d], at_x(e))

    for d in far:
        first_q(d).start()
    repeat(1, GY, lambda e: relay_q(0, e).start())
    for f in fetch[4:]:
        f.wait()
    joined = dot(lat_ref[...], w_ref[...], ((1,), (0,))).astype(BF16)
    for j in range(H):
        pk[j, :T, :] = joined[:, LANES * j : LANES * (j + 1)]
        pk[j, T:, :] = rot_ref[...]
    kb[x, a] = pk[a]
    for d in far:
        first_k(d).start()
    repeat(1, GX, lambda e: relay_k(0, e).start())
    lb[a] = lat_ref[...].reshape(lb.shape[1:])
    for d in far:
        first_q(d).wait_recv()
        repeat(1, GY, lambda e: relay_q(d, e).start())
    for d in far:
        first_k(d).wait_recv()
        repeat(1, GX, lambda e: relay_k(d, e).start())

    slab = T // TP
    mine = lat_ref.at[pl.ds(pl.multiple_of(tpi * slab, slab), slab)]

    def first_l(d):
        return copy(mine, lb.at[a, tpi], s1l.at[d - 1], r1l.at[d - 1], at_z(partner(H, a, d, 1)))

    def hand_on(d, i):
        piece = lb.at[partner(H, a, d, -1), tpi]
        return copy_tp(piece, piece, s8.at[d - 1, i - 1], r8.at[d - 1, i - 1], i)

    for d in far:
        first_l(d).start()

    many = GY * H * T

    def keys_of(where, units):
        tall, wide, turned = [], [], []
        for u in units:
            kv = kb[where, u, :T, :]
            rot = kb[where, u, T:, :]
            lane = lax.broadcasted_iota(jnp.int32, (T, LANES), 1)
            part = jnp.where(lane < NOPE, kv, jnp.zeros_like(kv))
            column = rot.astype(F32).T.astype(BF16)
            tall.append(jnp.concatenate([part, column, jnp.zeros((T, LANES - ROPE), BF16)], axis=1))
            wide.append(kv - part)
            turned.append(jnp.concatenate([kv.astype(F32).T.astype(BF16)[:NOPE], rot], axis=0))
        return jnp.concatenate(tall, axis=0), jnp.concatenate(wide, axis=0), jnp.concatenate(turned, axis=1)

    def attend(where, units):
        key, value, turned = keys_of(where, units)
        row = wq[:, :, :T, :].reshape(many, LANES)
        both = jnp.concatenate([row, rp[...]], axis=1)
        stats = [wq[i, j, T + quarter :, :].astype(F32) for i in range(GY) for j in range(H)]
        log = jnp.concatenate([t[0:1] + t[1:2] + t[2:3] for t in stats], axis=1)
        delta = jnp.concatenate([t[3:4] + t[4:5] + t[5:6] for t in stats], axis=1)
        s = dot(key, both, ((1,), (1,)))
        dp = dot(value, row, ((1,), (1,)))
        p = jnp.exp2(s * (scale * log2e) - log)
        ds = (p * (dp - delta)).astype(BF16)
        dq = dot(turned, ds, ((1,), (0,)))
        dk = dot(ds, both, ((1,), (0,))) * scale
        dv = dot(p.astype(BF16), row, ((1,), (0,)))
        lane = lax.broadcasted_iota(jnp.int32, dv.shape, 1)
        return dq, jnp.where(lane < NOPE, dk[:, :LANES], dv), dk[:, LANES:].T[:ROPE]

    for e in range(1, GY):
        for d in [0] + far:
            relay_q(d, e).wait_recv()
    for i in range(GY):
        for j in range(H):
            packed = wq[i, j, T : T + quarter, :]
            base = (i * H + j) * T
            for k in range(LANES // ROPE):
                part = packed if k == 0 else jnp.concatenate(
                    [packed[:, ROPE * k :], packed[:, : ROPE * k]], axis=1)
                rp[base + quarter * k : base + quarter * (k + 1), :] = part

    every = range(H)
    dq, kv, rot = attend(x, every)
    wide = H * T
    for i in range(GY):
        dqa[i] = dq[:, wide * i : wide * (i + 1)]
    own_kv[...] = kv
    own_rot[...] = rot

    order = [0] + far
    chunk = 2 if H % 2 == 0 else 1

    def back_k(e, n):
        piece = pl.ds(n * chunk, chunk)
        return copy(kvs.at[e - 1, piece], kvr.at[e - 1, piece], s3k.at[e - 1, n], r3k.at[e - 1, n], at_x(e))

    def unit_of(n, c, sign):
        return partner(H, a, order[n * chunk + c], sign)

    for e in range(1, GX):
        where = lax.rem(x + e, GX)
        for n in range(H // chunk):
            units = [unit_of(n, c, -1) for c in range(chunk)]
            for c in range(chunk):
                relay_k(order[n * chunk + c], GX - e).wait_recv()
            dq, kv, rot = attend(where, units)
            for c in range(chunk):
                kvs[e - 1, n * chunk + c, :T, :] = kv[T * c : T * (c + 1)].astype(KV_PART)
                kvs[e - 1, n * chunk + c, T:, :] = rot[:, T * c : T * (c + 1)].astype(KV_PART)
            back_k(e, n).start()
            for i in range(GY):
                dqa[i] += dq[:, wide * i : wide * (i + 1)]

    def back_q(e):
        return copy(dqs.at[e - 1], dqr.at[e - 1], s3q.at[e - 1], r3q.at[e - 1], at_y(e))

    for e in range(1, GY):
        dqs[e - 1] = dqa[lax.rem(y + e, GY)].astype(DQ_PART)
        back_q(e).start()

    for d in far:
        first_l(d).wait_recv()
        repeat(1, TP, lambda i: hand_on(d, i).start())

    def home_k(d):
        to = partner(H, a, d, 1)
        return copy(kvo.at[to], kvh.at[a], s4k.at[d - 1], r4k.at[d - 1], at_z(to))

    def home_r(d):
        to = partner(H, a, d, 1)
        return copy(ro.at[to], rr.at[a], s4r.at[d - 1], r4r.at[d - 1], at_z(to))

    for n in range(H // chunk):
        for e in range(1, GX):
            back_k(e, n).wait_recv()
        for c in range(chunk):
            slot = n * chunk + c
            u = unit_of(n, c, -1)
            place = pl.ds(pl.multiple_of(u * T, T), T)
            kvo[u] = (own_kv[place, :] + add_all([kvr[e - 1, slot, :T, :].astype(F32) for e in range(1, GX)])
                      if GX > 1 else own_kv[place, :]).astype(BF16)
            turn = own_rot[:, place]
            ro[u] = turn + add_all([kvr[e - 1, slot, T:, :].astype(F32) for e in range(1, GX)]) if GX > 1 else turn

    for d in far:
        home_k(d).start()
    kvh[a] = kvo[a]
    rr[a] = ro[a]

    for d in far:
        repeat(1, TP, lambda i: hand_on(d, i).wait_recv())
    lat = lb[...].reshape(wide, lb.shape[3])
    total = dot(lat, kvo[...].reshape(wide, LANES), ((0,), (0,)))
    rows = wgs.shape[1]
    wgs[...] = total.reshape(S, rows, LANES).astype(WG_PART)
    wgr[me] = wgs[me]

    def share(i):
        to = lax.rem(me + i, S)
        return copy(wgs.at[to], wgr.at[me], s5.at[i - 1], r5.at[i - 1], to)

    def spread(i, carry):
        share(i).start()
        return carry

    lax.fori_loop(1, S, spread, 0)
    for d in far:
        home_r(d).start()

    mine_q = dqa[y]
    for e in range(1, GY):
        back_q(e).wait_recv()
        mine_q = mine_q + dqr[e - 1].astype(F32)
    mine_q = (mine_q * scale).astype(BF16)
    for j in range(H):
        dqo[j] = mine_q[:, T * j : T * (j + 1)]

    def home_q(d):
        to = partner(H, a, d, 1)
        return copy(dqo.at[to], dqh.at[a], s4q.at[d - 1], r4q.at[d - 1], at_z(to))

    for d in far:
        home_q(d).start()
    dqh[a] = dqo[a]

    for d in far:
        home_k(d).wait_recv()
    for j in range(H):
        kg_ref[:, NOPE * j : NOPE * (j + 1)] = kvh[j, :, :NOPE]
        vg_ref[:, VDIM * j : VDIM * (j + 1)] = kvh[j, :, NOPE:]
    for d in far:
        home_r(d).wait_recv()
    rt[tpi] = add_all([rr[j] for j in range(H)])

    def swap(i):
        return copy_tp(rt.at[tpi], rt.at[tpi], s6.at[i - 1], r6.at[i - 1], i)

    repeat(1, TP, lambda i: swap(i).start())
    for d in far:
        home_q(d).wait_recv()
    qg_ref[...] = dqh[...].reshape(H * HEAD, T).astype(F32).T.astype(BF16)
    repeat(1, TP, lambda i: swap(i).wait_recv())
    rg_ref[...] = add_all([rt[i] for i in range(TP)])

    def arrive(i, carry):
        share(i).wait_recv()
        return carry

    lax.fori_loop(1, S, arrive, 0)
    for j in range(H):
        wg_ref[:, LANES * j : LANES * (j + 1)] = add_all([wgr[j * G + i].astype(F32) for i in range(G)])

    for d in far:
        for c in (first_q(d), first_k(d), first_l(d), home_k(d), home_r(d), home_q(d)):
            c.wait_send()
        repeat(1, TP, lambda i: hand_on(d, i).wait_send())
    for d in order:
        repeat(1, GY, lambda e: relay_q(d, e).wait_send())
        repeat(1, GX, lambda e: relay_k(d, e).wait_send())
    for n in range(H // chunk):
        repeat(1, GX, lambda e: back_k(e, n).wait_send())
    repeat(1, GY, lambda e: back_q(e).wait_send())
    repeat(1, TP, lambda i: swap(i).wait_send())

    def left(i, carry):
        share(i).wait_send()
        return carry

    lax.fori_loop(1, S, left, 0)


def put_out(*refs):
    copies = [pltpu.make_async_copy(refs[i], refs[5 + i], refs[10].at[i]) for i in range(5)]
    for c in copies:
        c.start()
    for c in copies:
        c.wait()


def per_device(S, TP, queries, latents, rot_key, kv_weight, log_sums, outputs, out_grad):
    T, rank = latents.shape
    H = log_sums.shape[1]
    G = S // H
    GX = max(d for d in range(1, math.isqrt(G) + 1) if G % d == 0)
    GY = G // GX
    rows = rank // S
    wide = H * T
    dma = lambda *n: pltpu.SemaphoreType.DMA(tuple(max(k, 1) for k in n))
    pairs = lambda *n: [dma(*n), dma(*n)]
    vm = lambda shape, kind: pltpu.VMEM(tuple(max(k, 1) for k in shape), kind)
    unit = T + T * ROPE // LANES + STATS
    arrays = (queries, latents, rot_key.T, kv_weight, log_sums.T, outputs, out_grad)
    scratch = [
        *[vm(u.shape, u.dtype) for u in arrays], dma(len(arrays)),
        vm((H, unit, LANES), BF16), vm((H, T + ROPE, LANES), BF16),
        vm((GY, H, unit, LANES), BF16), vm((GX, H, T + ROPE, LANES), BF16), vm((H, TP, T // TP, rank), BF16),
        vm((GY * wide, LANES), BF16), vm((GY, HEAD, wide), F32),
        *[vm((GY - 1, HEAD, wide), DQ_PART)] * 2, *[vm((GX - 1, H, T + ROPE, LANES), KV_PART)] * 2,
        vm((wide, LANES), F32), vm((ROPE, wide), F32),
        *[vm((H, T, LANES), BF16)] * 2, *[vm((H, ROPE, T), F32)] * 2, vm((TP, ROPE, T), F32),
        *[vm((S, rows, LANES), WG_PART)] * 2, *[vm((H, HEAD, T), BF16)] * 2,
        *pairs(H - 1), *pairs(H - 1), *pairs(H - 1), *pairs(GY - 1, H), *pairs(GX - 1, H),
        *pairs(GY - 1), *pairs(GX - 1, H),
        *pairs(H - 1), *pairs(H - 1), *pairs(H - 1), *pairs(S - 1), *pairs(TP - 1), *pairs(H - 1, TP - 1),
    ]
    shapes = [
        ((T, H * HEAD), BF16), ((T, H * NOPE), BF16), ((T, H * VDIM), BF16),
        ((ROPE, T), F32), ((rows, H * LANES), F32),
    ]
    held = sum(u[0] * -(-u[1] // LANES) * LANES * jnp.dtype(t).itemsize for u, t in shapes)
    results = pl.pallas_call(
        functools.partial(kernel, S, TP, H, GY, GX),
        out_shape=[pltpu.VMEM(*u) for u in shapes],
        in_specs=[pl.BlockSpec(memory_space=pltpu.HBM)] * 7,
        out_specs=[pl.BlockSpec(memory_space=pltpu.VMEM)] * 5,
        scratch_shapes=scratch,
        compiler_params=pltpu.CompilerParams(
            collective_id=0, has_side_effects=True, vmem_limit_bytes=VMEM_BYTES - held - SPARE
        ),
    )(*arrays)
    query_grad, key_grad, value_grad, rot_grad, weight_grad = pl.pallas_call(
        put_out,
        out_shape=[jax.ShapeDtypeStruct(*u) for u in shapes],
        in_specs=[pl.BlockSpec(memory_space=pltpu.VMEM)] * 5,
        out_specs=[pl.BlockSpec(memory_space=pltpu.HBM)] * 5,
        scratch_shapes=[dma(5)],
        compiler_params=pltpu.CompilerParams(vmem_limit_bytes=1 << 20),
    )(*results)
    return query_grad, key_grad, value_grad, rot_grad.T, weight_grad


def solution(mesh):
    placed = (
        P("sp", "tp"), P("sp", None), P("sp", None), P(None, "tp"),
        P("sp", "tp"), P("sp", "tp"), P("sp", "tp"),
    )
    return jax.shard_map(
        functools.partial(per_device, mesh.shape["sp"], mesh.shape["tp"]),
        mesh=mesh,
        in_specs=placed,
        out_specs=(P("sp", "tp"), P("sp", "tp"), P("sp", "tp"), P("sp", None), P("sp", "tp")),
        check_vma=False,
    )
```

```python
import functools
import math

import jax
import jax.numpy as jnp
from jax import lax
from jax.experimental import pallas as pl
from jax.experimental.pallas import tpu as pltpu
from jax.sharding import PartitionSpec as P

NOPE = 64
ROPE = 32
VDIM = 64
HEAD = NOPE + ROPE
LANES = 128
STATS = 8
VMEM_BYTES = 67043328
SPARE = 8192
MESH = pl.DeviceIdType.MESH
F32 = jnp.float32
BF16 = jnp.bfloat16
KV_PART = BF16
DQ_PART = BF16
WG_PART = BF16


def dot(x, y, dims):
    return lax.dot_general(x, y, (dims, ((), ())), preferred_element_type=F32)


def three_terms(x):
    hi = x.astype(BF16)
    rest = x - hi.astype(F32)
    mid = rest.astype(BF16)
    low = (rest - mid.astype(F32)).astype(BF16)
    return hi, mid, low


def repeat(start, stop, body):
    if stop - start <= 4:
        for i in range(start, stop):
            body(i)
    else:
        def step(i, carry):
            body(i)
            return carry

        lax.fori_loop(start, stop, step, 0)


def add_all(terms):
    return functools.reduce(lambda x, y: x + y, terms)


def power_of_two(n):
    return n & (n - 1) == 0


def partner(n, i, d, sign):
    if not power_of_two(n):
        return lax.rem(i + sign * d + n, n)
    bit = 1
    result = i
    while bit <= d:
        if d & bit:
            result = result + bit * (1 - 2 * lax.rem(i // bit, 2))
        bit *= 2
    return result


def distances(n):
    if not power_of_two(n):
        return list(range(1, n))
    return sorted(range(1, n), key=lambda d: -bin(d).count("1"))


def kernel(
    S, TP, H, GY, GX,
    q_in, lat_in, rot_in, w_in, log_in, out_in, go_in,
    qg_ref, kg_ref, vg_ref, rg_ref, wg_ref,
    q_ref, lat_ref, rot_ref, w_ref, log_ref, out_ref, go_ref, loads,
    qs, pk, wq, kb, lb, rp, dqa, dqs, dqr, kvs, kvr, dka, dva,
    kvo, kvh, ro, rr, rt, wgs, wgr, dqo, dqh,
    s1q, r1q, s1k, r1k, s1l, r1l, s2q, r2q, s2k, r2k, s3q, r3q, s3k, r3k,
    s4q, r4q, s4k, r4k, s4r, r4r, s5, r5, s6, r6, s8, r8,
):
    G = GY * GX
    T = q_ref.shape[0]
    me = lax.axis_index("sp")
    tpi = lax.axis_index("tp")
    a, b = lax.rem(me, H), me // H
    y, x = b // GX, lax.rem(b, GX)
    scale = HEAD ** (-0.5)
    log2e = math.log2(math.e)
    far = distances(H)
    quarter = T * ROPE // LANES

    barrier = pltpu.get_barrier_semaphore()

    def greet(to):
        pl.semaphore_signal(barrier, inc=1, device_id={"sp": to}, device_id_type=MESH)

    def greet_tp(i):
        pl.semaphore_signal(barrier, inc=1, device_id={"tp": lax.rem(tpi + i, TP)}, device_id_type=MESH)

    def at_a(z):
        return b * H + z

    def at_y(e):
        return (lax.rem(y + e, GY) * GX + x) * H + a

    def at_x(e):
        return (y * GX + lax.rem(x + e, GX)) * H + a

    pairs = (
        (q_in, q_ref), (go_in, go_ref), (out_in, out_ref), (log_in, log_ref),
        (lat_in, lat_ref), (w_in, w_ref), (rot_in, rot_ref),
    )
    fetch = [pltpu.make_async_copy(u, v, loads.at[i]) for i, (u, v) in enumerate(pairs)]
    for f in fetch:
        f.start()
    for d in far:
        greet(at_a(partner(H, a, d, 1)))
    repeat(1, GY, lambda e: greet(at_y(e)))
    repeat(1, GX, lambda e: greet(at_x(e)))
    repeat(1, TP, greet_tp)

    def copy(src, dst, ssem, rsem, sp):
        return pltpu.make_async_remote_copy(
            src_ref=src, dst_ref=dst, send_sem=ssem, recv_sem=rsem,
            device_id={"sp": sp}, device_id_type=MESH,
        )

    def copy_tp(src, dst, ssem, rsem, i):
        return pltpu.make_async_remote_copy(
            src_ref=src, dst_ref=dst, send_sem=ssem, recv_sem=rsem,
            device_id={"tp": lax.rem(tpi + i, TP)}, device_id_type=MESH,
        )

    for f in fetch[:4]:
        f.wait()
    prod = out_ref[...].astype(F32) * go_ref[...].astype(F32)
    high = prod.astype(BF16)
    rest = (prod - high.astype(F32)).astype(BF16)
    head_of = lax.broadcasted_iota(jnp.int32, (8 * -(-H // 8), H * VDIM), 1) // VDIM
    picks = (head_of == lax.broadcasted_iota(jnp.int32, head_of.shape, 0)).astype(F32).astype(BF16)
    deltas = dot(picks, high, ((1,), (1,))) + dot(picks, rest, ((1,), (1,)))
    logs = log_ref[...] * log2e
    for j in range(H):
        start = HEAD * j
        qs[j, :T, :] = jnp.concatenate(
            [q_ref[:, start : start + NOPE], go_ref[:, VDIM * j : VDIM * (j + 1)]], axis=1)
        turned = q_ref[:, start + NOPE : start + HEAD]
        qs[j, T : T + quarter, :] = jnp.concatenate(
            [turned[quarter * i : quarter * (i + 1)] for i in range(LANES // ROPE)], axis=1)
        terms = three_terms(logs[j : j + 1]) + three_terms(deltas[j : j + 1])
        qs[j, T + quarter :, :] = jnp.concatenate(
            [t.astype(F32) for t in terms] + [jnp.zeros((STATS - 6, T), F32)], axis=0).astype(BF16)
    wq[y, a] = qs[a]
    pl.semaphore_wait(barrier, H - 1 + GY - 1 + GX - 1 + TP - 1)

    def first_q(d):
        to = partner(H, a, d, 1)
        return copy(qs.at[to], wq.at[y, a], s1q.at[d - 1], r1q.at[d - 1], at_a(to))

    def first_k(d):
        to = partner(H, a, d, 1)
        return copy(pk.at[to], kb.at[x, a], s1k.at[d - 1], r1k.at[d - 1], at_a(to))

    def relay_q(d, e):
        src = wq.at[y, partner(H, a, d, -1)]
        return copy(src, src, s2q.at[e - 1, d], r2q.at[e - 1, d], at_y(e))

    def relay_k(d, e):
        src = kb.at[x, partner(H, a, d, -1)]
        return copy(src, src, s2k.at[e - 1, d], r2k.at[e - 1, d], at_x(e))

    for d in far:
        first_q(d).start()
    repeat(1, GY, lambda e: relay_q(0, e).start())
    for f in fetch[4:]:
        f.wait()
    joined = dot(lat_ref[...], w_ref[...], ((1,), (0,))).astype(BF16)
    for j in range(H):
        pk[j, :T, :] = joined[:, LANES * j : LANES * (j + 1)]
        pk[j, T:, :] = rot_ref[...]
    kb[x, a] = pk[a]
    for d in far:
        first_k(d).start()
    repeat(1, GX, lambda e: relay_k(0, e).start())
    lb[a] = lat_ref[...].reshape(lb.shape[1:])
    for d in far:
        first_q(d).wait_recv()
        repeat(1, GY, lambda e: relay_q(d, e).start())
    for d in far:
        first_k(d).wait_recv()
        repeat(1, GX, lambda e: relay_k(d, e).start())

    slab = T // TP
    mine = lat_ref.at[pl.ds(pl.multiple_of(tpi * slab, slab), slab)]

    def first_l(d):
        return copy(mine, lb.at[a, tpi], s1l.at[d - 1], r1l.at[d - 1], at_a(partner(H, a, d, 1)))

    def hand_on(d, i):
        piece = lb.at[partner(H, a, d, -1), tpi]
        return copy_tp(piece, piece, s8.at[d - 1, i - 1], r8.at[d - 1, i - 1], i)

    for d in far:
        first_l(d).start()

    def keys_of(e, units):
        where = lax.rem(x + e, GX)
        tall, wide, turned = [], [], []
        for u in units:
            kv = kb[where, u, :T, :]
            rot = kb[where, u, T:, :]
            lane = lax.broadcasted_iota(jnp.int32, (T, LANES), 1)
            part = jnp.where(lane < NOPE, kv, jnp.zeros_like(kv))
            column = rot.astype(F32).T.astype(BF16)
            tall.append(jnp.concatenate([part, column, jnp.zeros((T, LANES - ROPE), BF16)], axis=1))
            wide.append(kv - part)
            turned.append(jnp.concatenate([kv.astype(F32).T.astype(BF16)[:NOPE], rot], axis=0))
        return jnp.concatenate(tall, axis=0), jnp.concatenate(wide, axis=0), jnp.concatenate(turned, axis=1)

    wide = H * T
    order = [0] + far
    chunk = 2 if H % 2 == 0 else 1
    chunks = H // chunk

    def prepare(f):
        col = lax.rem(y + f, GY)
        for j in range(H):
            packed = wq[col, j, T : T + quarter, :]
            for k in range(LANES // ROPE):
                part = packed if k == 0 else jnp.concatenate(
                    [packed[:, ROPE * k :], packed[:, : ROPE * k]], axis=1)
                rp[f, T * j + quarter * k : T * j + quarter * (k + 1), :] = part

    def attend(keys, f):
        key, value, turned = keys
        col = lax.rem(y + f, GY)
        row = wq[col, :, :T, :].reshape(wide, LANES)
        both = jnp.concatenate([row, rp[f]], axis=1)
        stats = [wq[col, j, T + quarter :, :].astype(F32) for j in range(H)]
        log = jnp.concatenate([t[0:1] + t[1:2] + t[2:3] for t in stats], axis=1)
        delta = jnp.concatenate([t[3:4] + t[4:5] + t[5:6] for t in stats], axis=1)
        s = dot(key, both, ((1,), (1,)))
        dp = dot(value, row, ((1,), (1,)))
        p = jnp.exp2(s * (scale * log2e) - log)
        ds = (p * (dp - delta)).astype(BF16)
        dq = dot(turned, ds, ((1,), (0,)))
        dk = dot(ds, both, ((1,), (0,)))
        dv = dot(p.astype(BF16), row, ((1,), (0,)))
        return dq, dk, dv

    def unit_of(k, sign):
        return partner(H, a, order[k], sign)

    def span(n):
        return pl.ds(wide // chunks * n, wide // chunks)

    def keys_at(e, n):
        return keys_of(e, [unit_of(n * chunk + c, -1) for c in range(chunk)])

    def whole_keys(e):
        return keys_of(e, [unit_of(k, -1) for k in range(H)])

    def gather(e, n, dk, dv, first):
        if first:
            dka[e, span(n), :] = dk
            dva[e, span(n), :] = dv
        else:
            dka[e, span(n), :] += dk
            dva[e, span(n), :] += dv

    def gather_all(e, dk, dv, first):
        for n in range(chunks):
            part = slice(wide // chunks * n, wide // chunks * (n + 1))
            gather(e, n, dk[part], dv[part], first)

    def totals(e, n):
        dk, dv = dka[e, span(n), :], dva[e, span(n), :]
        lane = lax.broadcasted_iota(jnp.int32, dv.shape, 1)
        dk = dk * scale
        return jnp.where(lane < NOPE, dk[:, :LANES], dv), dk[:, LANES:].T[:ROPE]

    def back_k(e, n):
        piece = pl.ds(n * chunk, chunk)
        return copy(kvs.at[e - 1, piece], kvr.at[e - 1, piece], s3k.at[e - 1, n], r3k.at[e - 1, n], at_x(e))

    def back_q(f):
        return copy(dqs.at[f - 1], dqr.at[f - 1], s3q.at[f - 1], r3q.at[f - 1], at_y(f))

    def send_k(e, n):
        kv, rot = totals(e, n)
        for c in range(chunk):
            kvs[e - 1, n * chunk + c, :T, :] = kv[T * c : T * (c + 1)].astype(KV_PART)
            kvs[e - 1, n * chunk + c, T:, :] = rot[:, T * c : T * (c + 1)].astype(KV_PART)
        back_k(e, n).start()

    prepare(0)
    dq, dk, dv = attend(whole_keys(0), 0)
    dqa[0] = dq
    gather_all(0, dk, dv, True)
    for e in range(1, GX):
        for d in order:
            relay_k(d, GX - e).wait_recv()
        dq, dk, dv = attend(whole_keys(e), 0)
        dqa[0] += dq
        gather_all(e, dk, dv, True)
    for f in range(1, GY):
        for d in order:
            relay_q(d, GY - f).wait_recv()
        prepare(f)
        for e in range(1, GX):
            for n in range(chunks):
                dq, dk, dv = attend(keys_at(e, n), f)
                if e == 1 and n == 0:
                    dqa[f] = dq
                else:
                    dqa[f] += dq
                gather(e, n, dk, dv, False)
                if f == GY - 1:
                    send_k(e, n)
        dq, dk, dv = attend(whole_keys(0), f)
        dqs[f - 1] = (dqa[f] + dq if GX > 1 else dq).astype(DQ_PART)
        back_q(f).start()
        gather_all(0, dk, dv, False)

    for d in far:
        first_l(d).wait_recv()
        repeat(1, TP, lambda i: hand_on(d, i).start())

    def home_k(d):
        to = partner(H, a, d, -1)
        return copy(kvo.at[order.index(d)], kvh.at[a], s4k.at[d - 1], r4k.at[d - 1], at_a(to))

    def home_r(d):
        to = partner(H, a, d, -1)
        return copy(ro.at[order.index(d)], rr.at[a], s4r.at[d - 1], r4r.at[d - 1], at_a(to))

    for d in far:
        repeat(1, TP, lambda i: hand_on(d, i).wait_recv())
    grads = []
    for n in range(chunks):
        for e in range(1, GX):
            back_k(e, n).wait_recv()
        kv, rot = totals(0, n)
        lats, finals = [], []
        for c in range(chunk):
            slot = n * chunk + c
            u = unit_of(slot, -1)
            part, turn = kv[T * c : T * (c + 1)], rot[:, T * c : T * (c + 1)]
            for e in range(1, GX):
                part = part + kvr[e - 1, slot, :T, :].astype(F32)
                turn = turn + kvr[e - 1, slot, T:, :].astype(F32)
            part = part.astype(BF16)
            kvo[slot] = part
            ro[slot] = turn
            lats.append(lb[u].reshape(T, lb.shape[3]))
            finals.append(part)
            if slot == 0:
                kvh[a] = part
                rr[a] = turn
            else:
                home_k(order[slot]).start()
        grads.append(dot(jnp.concatenate(lats, axis=0), jnp.concatenate(finals, axis=0), ((0,), (0,))))
    total = add_all(grads)
    rows = wgs.shape[1]
    wgs[...] = total.reshape(S, rows, LANES).astype(WG_PART)
    wgr[me] = wgs[me]

    def share(i):
        to = lax.rem(me + i, S)
        return copy(wgs.at[to], wgr.at[me], s5.at[i - 1], r5.at[i - 1], to)

    def spread(i, carry):
        share(i).start()
        return carry

    lax.fori_loop(1, S, spread, 0)
    for d in far:
        home_r(d).start()

    mine_q = dqa[0]
    for e in range(1, GY):
        back_q(e).wait_recv()
        mine_q = mine_q + dqr[e - 1].astype(F32)
    mine_q = (mine_q * scale).astype(BF16)
    for j in range(H):
        dqo[j] = mine_q[:, T * j : T * (j + 1)]

    def home_q(d):
        to = partner(H, a, d, 1)
        return copy(dqo.at[to], dqh.at[a], s4q.at[d - 1], r4q.at[d - 1], at_a(to))

    for d in far:
        home_q(d).start()
    dqh[a] = dqo[a]

    for d in far:
        home_k(d).wait_recv()
    for j in range(H):
        kg_ref[:, NOPE * j : NOPE * (j + 1)] = kvh[j, :, :NOPE]
        vg_ref[:, VDIM * j : VDIM * (j + 1)] = kvh[j, :, NOPE:]
    for d in far:
        home_r(d).wait_recv()
    rt[tpi] = add_all([rr[j] for j in range(H)])

    def swap(i):
        return copy_tp(rt.at[tpi], rt.at[tpi], s6.at[i - 1], r6.at[i - 1], i)

    repeat(1, TP, lambda i: swap(i).start())
    for d in far:
        home_q(d).wait_recv()
    qg_ref[...] = dqh[...].reshape(H * HEAD, T).astype(F32).T.astype(BF16)
    repeat(1, TP, lambda i: swap(i).wait_recv())
    rg_ref[...] = add_all([rt[i] for i in range(TP)])

    def arrive(i, carry):
        share(i).wait_recv()
        return carry

    lax.fori_loop(1, S, arrive, 0)
    for j in range(H):
        wg_ref[:, LANES * j : LANES * (j + 1)] = add_all([wgr[i * H + j].astype(F32) for i in range(G)])

    for d in far:
        for c in (first_q(d), first_k(d), first_l(d), home_k(d), home_r(d), home_q(d)):
            c.wait_send()
        repeat(1, TP, lambda i: hand_on(d, i).wait_send())
    for d in order:
        repeat(1, GY, lambda e: relay_q(d, e).wait_send())
        repeat(1, GX, lambda e: relay_k(d, e).wait_send())
    for n in range(chunks):
        repeat(1, GX, lambda e: back_k(e, n).wait_send())
    repeat(1, GY, lambda e: back_q(e).wait_send())
    repeat(1, TP, lambda i: swap(i).wait_send())

    def left(i, carry):
        share(i).wait_send()
        return carry

    lax.fori_loop(1, S, left, 0)


def put_out(*refs):
    copies = [pltpu.make_async_copy(refs[i], refs[5 + i], refs[10].at[i]) for i in range(5)]
    for c in copies:
        c.start()
    for c in copies:
        c.wait()


def per_device(S, TP, queries, latents, rot_key, kv_weight, log_sums, outputs, out_grad):
    T, rank = latents.shape
    H = log_sums.shape[1]
    G = S // H
    GX = max(d for d in range(1, math.isqrt(G) + 1) if G % d == 0)
    GY = G // GX
    rows = rank // S
    wide = H * T
    dma = lambda *n: pltpu.SemaphoreType.DMA(tuple(max(k, 1) for k in n))
    pairs = lambda *n: [dma(*n), dma(*n)]
    vm = lambda shape, kind: pltpu.VMEM(tuple(max(k, 1) for k in shape), kind)
    unit = T + T * ROPE // LANES + STATS
    arrays = (queries, latents, rot_key.T, kv_weight, log_sums.T, outputs, out_grad)
    scratch = [
        *[vm(u.shape, u.dtype) for u in arrays], dma(len(arrays)),
        vm((H, unit, LANES), BF16), vm((H, T + ROPE, LANES), BF16),
        vm((GY, H, unit, LANES), BF16), vm((GX, H, T + ROPE, LANES), BF16), vm((H, TP, T // TP, rank), BF16),
        vm((GY, wide, LANES), BF16), vm((GY, HEAD, wide), F32),
        *[vm((GY - 1, HEAD, wide), DQ_PART)] * 2, *[vm((GX - 1, H, T + ROPE, LANES), KV_PART)] * 2,
        vm((GX, wide, 2 * LANES), F32), vm((GX, wide, LANES), F32),
        *[vm((H, T, LANES), BF16)] * 2, *[vm((H, ROPE, T), F32)] * 2, vm((TP, ROPE, T), F32),
        *[vm((S, rows, LANES), WG_PART)] * 2, *[vm((H, HEAD, T), BF16)] * 2,
        *pairs(H - 1), *pairs(H - 1), *pairs(H - 1), *pairs(GY - 1, H), *pairs(GX - 1, H),
        *pairs(GY - 1), *pairs(GX - 1, H),
        *pairs(H - 1), *pairs(H - 1), *pairs(H - 1), *pairs(S - 1), *pairs(TP - 1), *pairs(H - 1, TP - 1),
    ]
    shapes = [
        ((T, H * HEAD), BF16), ((T, H * NOPE), BF16), ((T, H * VDIM), BF16),
        ((ROPE, T), F32), ((rows, H * LANES), F32),
    ]
    held = sum(u[0] * -(-u[1] // LANES) * LANES * jnp.dtype(t).itemsize for u, t in shapes)
    results = pl.pallas_call(
        functools.partial(kernel, S, TP, H, GY, GX),
        out_shape=[pltpu.VMEM(*u) for u in shapes],
        in_specs=[pl.BlockSpec(memory_space=pltpu.HBM)] * 7,
        out_specs=[pl.BlockSpec(memory_space=pltpu.VMEM)] * 5,
        scratch_shapes=scratch,
        compiler_params=pltpu.CompilerParams(
            collective_id=0, has_side_effects=True, vmem_limit_bytes=VMEM_BYTES - held - SPARE
        ),
    )(*arrays)
    query_grad, key_grad, value_grad, rot_grad, weight_grad = pl.pallas_call(
        put_out,
        out_shape=[jax.ShapeDtypeStruct(*u) for u in shapes],
        in_specs=[pl.BlockSpec(memory_space=pltpu.VMEM)] * 5,
        out_specs=[pl.BlockSpec(memory_space=pltpu.HBM)] * 5,
        scratch_shapes=[dma(5)],
        compiler_params=pltpu.CompilerParams(vmem_limit_bytes=1 << 20),
    )(*results)
    return query_grad, key_grad, value_grad, rot_grad.T, weight_grad


def solution(mesh):
    placed = (
        P("sp", "tp"), P("sp", None), P("sp", None), P(None, "tp"),
        P("sp", "tp"), P("sp", "tp"), P("sp", "tp"),
    )
    return jax.shard_map(
        functools.partial(per_device, mesh.shape["sp"], mesh.shape["tp"]),
        mesh=mesh,
        in_specs=placed,
        out_specs=(P("sp", "tp"), P("sp", "tp"), P("sp", "tp"), P("sp", None), P("sp", "tp")),
        check_vma=False,
    )
```

```python
import functools
import math

import jax
import jax.numpy as jnp
from jax import lax
from jax.experimental import pallas as pl
from jax.experimental.pallas import tpu as pltpu
from jax.sharding import PartitionSpec as P

NOPE = 64
ROPE = 32
VDIM = 64
HEAD = NOPE + ROPE
LANES = 128
STATS = 8
VMEM_BYTES = 67043328
SPARE = 8192
MESH = pl.DeviceIdType.MESH
F32 = jnp.float32
BF16 = jnp.bfloat16
KV_PART = BF16
DQ_PART = BF16
WG_PART = BF16


def dot(x, y, dims):
    return lax.dot_general(x, y, (dims, ((), ())), preferred_element_type=F32)


def three_terms(x):
    hi = x.astype(BF16)
    rest = x - hi.astype(F32)
    mid = rest.astype(BF16)
    low = (rest - mid.astype(F32)).astype(BF16)
    return hi, mid, low


def repeat(start, stop, body):
    if stop - start <= 4:
        for i in range(start, stop):
            body(i)
    else:
        def step(i, carry):
            body(i)
            return carry

        lax.fori_loop(start, stop, step, 0)


def add_all(terms):
    return functools.reduce(lambda x, y: x + y, terms)


def power_of_two(n):
    return n & (n - 1) == 0


def partner(n, i, d, sign):
    if not power_of_two(n):
        return lax.rem(i + sign * d + n, n)
    bit = 1
    result = i
    while bit <= d:
        if d & bit:
            result = result + bit * (1 - 2 * lax.rem(i // bit, 2))
        bit *= 2
    return result


def distances(n):
    if not power_of_two(n):
        return list(range(1, n))
    return sorted(range(1, n), key=lambda d: -bin(d).count("1"))


def general_kernel(
    S, TP, H, GY, GX,
    q_in, lat_in, rot_in, w_in, log_in, out_in, go_in,
    qg_ref, kg_ref, vg_ref, rg_ref, wg_ref,
    q_ref, lat_ref, rot_ref, w_ref, log_ref, out_ref, go_ref, loads,
    qs, pk, wq, kb, lb, rp, dqa, dqs, dqr, kvs, kvr, dka, dva,
    kvo, kvh, ro, rr, rt, wgs, wgr, dqo, dqh,
    s1q, r1q, s1k, r1k, s1l, r1l, s2q, r2q, s2k, r2k, s3q, r3q, s3k, r3k,
    s4q, r4q, s4k, r4k, s4r, r4r, s5, r5, s6, r6, s8, r8,
):
    G = GY * GX
    T = q_ref.shape[0]
    me = lax.axis_index("sp")
    tpi = lax.axis_index("tp")
    a, b = lax.rem(me, H), me // H
    y, x = b // GX, lax.rem(b, GX)
    scale = HEAD ** (-0.5)
    log2e = math.log2(math.e)
    far = distances(H)
    quarter = T * ROPE // LANES

    barrier = pltpu.get_barrier_semaphore()

    def greet(to):
        pl.semaphore_signal(barrier, inc=1, device_id={"sp": to}, device_id_type=MESH)

    def greet_tp(i):
        pl.semaphore_signal(barrier, inc=1, device_id={"tp": lax.rem(tpi + i, TP)}, device_id_type=MESH)

    def at_a(z):
        return b * H + z

    def at_y(e):
        return (lax.rem(y + e, GY) * GX + x) * H + a

    def at_x(e):
        return (y * GX + lax.rem(x + e, GX)) * H + a

    pairs = (
        (q_in, q_ref), (go_in, go_ref), (out_in, out_ref), (log_in, log_ref),
        (lat_in, lat_ref), (w_in, w_ref), (rot_in, rot_ref),
    )
    fetch = [pltpu.make_async_copy(u, v, loads.at[i]) for i, (u, v) in enumerate(pairs)]
    for f in fetch:
        f.start()
    for d in far:
        greet(at_a(partner(H, a, d, 1)))
    repeat(1, GY, lambda e: greet(at_y(e)))
    repeat(1, GX, lambda e: greet(at_x(e)))
    repeat(1, TP, greet_tp)

    def copy(src, dst, ssem, rsem, sp):
        return pltpu.make_async_remote_copy(
            src_ref=src, dst_ref=dst, send_sem=ssem, recv_sem=rsem,
            device_id={"sp": sp}, device_id_type=MESH,
        )

    def copy_tp(src, dst, ssem, rsem, i):
        return pltpu.make_async_remote_copy(
            src_ref=src, dst_ref=dst, send_sem=ssem, recv_sem=rsem,
            device_id={"tp": lax.rem(tpi + i, TP)}, device_id_type=MESH,
        )

    for f in fetch[:4]:
        f.wait()
    prod = out_ref[...].astype(F32) * go_ref[...].astype(F32)
    high = prod.astype(BF16)
    rest = (prod - high.astype(F32)).astype(BF16)
    head_of = lax.broadcasted_iota(jnp.int32, (8 * -(-H // 8), H * VDIM), 1) // VDIM
    picks = (head_of == lax.broadcasted_iota(jnp.int32, head_of.shape, 0)).astype(F32).astype(BF16)
    deltas = dot(picks, high, ((1,), (1,))) + dot(picks, rest, ((1,), (1,)))
    logs = log_ref[...] * log2e
    for j in range(H):
        start = HEAD * j
        qs[j, :T, :] = jnp.concatenate(
            [q_ref[:, start : start + NOPE], go_ref[:, VDIM * j : VDIM * (j + 1)]], axis=1)
        turned = q_ref[:, start + NOPE : start + HEAD]
        qs[j, T : T + quarter, :] = jnp.concatenate(
            [turned[quarter * i : quarter * (i + 1)] for i in range(LANES // ROPE)], axis=1)
        terms = three_terms(logs[j : j + 1]) + three_terms(deltas[j : j + 1])
        qs[j, T + quarter :, :] = jnp.concatenate(
            [t.astype(F32) for t in terms] + [jnp.zeros((STATS - 6, T), F32)], axis=0).astype(BF16)
    wq[y, a] = qs[a]
    pl.semaphore_wait(barrier, H - 1 + GY - 1 + GX - 1 + TP - 1)

    def first_q(d):
        to = partner(H, a, d, 1)
        return copy(qs.at[to], wq.at[y, a], s1q.at[d - 1], r1q.at[d - 1], at_a(to))

    def first_k(d):
        to = partner(H, a, d, 1)
        return copy(pk.at[to], kb.at[x, a], s1k.at[d - 1], r1k.at[d - 1], at_a(to))

    def relay_q(d, e):
        src = wq.at[y, partner(H, a, d, -1)]
        return copy(src, src, s2q.at[e - 1, d], r2q.at[e - 1, d], at_y(e))

    def relay_k(d, e):
        src = kb.at[x, partner(H, a, d, -1)]
        return copy(src, src, s2k.at[e - 1, d], r2k.at[e - 1, d], at_x(e))

    for d in far:
        first_q(d).start()
    repeat(1, GY, lambda e: relay_q(0, e).start())
    for f in fetch[4:]:
        f.wait()
    joined = dot(lat_ref[...], w_ref[...], ((1,), (0,))).astype(BF16)
    for j in range(H):
        pk[j, :T, :] = joined[:, LANES * j : LANES * (j + 1)]
        pk[j, T:, :] = rot_ref[...]
    kb[x, a] = pk[a]
    for d in far:
        first_k(d).start()
    repeat(1, GX, lambda e: relay_k(0, e).start())
    lb[a] = lat_ref[...].reshape(lb.shape[1:])
    for d in far:
        first_q(d).wait_recv()
        repeat(1, GY, lambda e: relay_q(d, e).start())
    for d in far:
        first_k(d).wait_recv()
        repeat(1, GX, lambda e: relay_k(d, e).start())

    slab = T // TP
    mine = lat_ref.at[pl.ds(pl.multiple_of(tpi * slab, slab), slab)]

    def first_l(d):
        return copy(mine, lb.at[a, tpi], s1l.at[d - 1], r1l.at[d - 1], at_a(partner(H, a, d, 1)))

    def hand_on(d, i):
        piece = lb.at[partner(H, a, d, -1), tpi]
        return copy_tp(piece, piece, s8.at[d - 1, i - 1], r8.at[d - 1, i - 1], i)

    for d in far:
        first_l(d).start()

    def keys_of(e, units):
        where = lax.rem(x + e, GX)
        tall, wide, turned = [], [], []
        for u in units:
            kv = kb[where, u, :T, :]
            rot = kb[where, u, T:, :]
            lane = lax.broadcasted_iota(jnp.int32, (T, LANES), 1)
            part = jnp.where(lane < NOPE, kv, jnp.zeros_like(kv))
            column = rot.astype(F32).T.astype(BF16)
            tall.append(jnp.concatenate([part, column, jnp.zeros((T, LANES - ROPE), BF16)], axis=1))
            wide.append(kv - part)
            turned.append(jnp.concatenate([kv.astype(F32).T.astype(BF16)[:NOPE], rot], axis=0))
        return jnp.concatenate(tall, axis=0), jnp.concatenate(wide, axis=0), jnp.concatenate(turned, axis=1)

    wide = H * T
    order = [0] + far
    chunk = 2 if H % 2 == 0 else 1
    chunks = H // chunk

    def prepare(f):
        col = lax.rem(y + f, GY)
        for j in range(H):
            packed = wq[col, j, T : T + quarter, :]
            for k in range(LANES // ROPE):
                part = packed if k == 0 else jnp.concatenate(
                    [packed[:, ROPE * k :], packed[:, : ROPE * k]], axis=1)
                rp[f, T * j + quarter * k : T * j + quarter * (k + 1), :] = part

    def attend(keys, f):
        key, value, turned = keys
        col = lax.rem(y + f, GY)
        row = wq[col, :, :T, :].reshape(wide, LANES)
        both = jnp.concatenate([row, rp[f]], axis=1)
        stats = [wq[col, j, T + quarter :, :].astype(F32) for j in range(H)]
        log = jnp.concatenate([t[0:1] + t[1:2] + t[2:3] for t in stats], axis=1)
        delta = jnp.concatenate([t[3:4] + t[4:5] + t[5:6] for t in stats], axis=1)
        s = dot(key, both, ((1,), (1,)))
        dp = dot(value, row, ((1,), (1,)))
        p = jnp.exp2(s * (scale * log2e) - log)
        ds = (p * (dp - delta)).astype(BF16)
        dq = dot(turned, ds, ((1,), (0,)))
        dk = dot(ds, both, ((1,), (0,)))
        dv = dot(p.astype(BF16), row, ((1,), (0,)))
        return dq, dk, dv

    def unit_of(k, sign):
        return partner(H, a, order[k], sign)

    def span(n):
        return pl.ds(wide // chunks * n, wide // chunks)

    def keys_at(e, n):
        return keys_of(e, [unit_of(n * chunk + c, -1) for c in range(chunk)])

    def whole_keys(e):
        return keys_of(e, [unit_of(k, -1) for k in range(H)])

    def gather(e, n, dk, dv, first):
        if first:
            dka[e, span(n), :] = dk
            dva[e, span(n), :] = dv
        else:
            dka[e, span(n), :] += dk
            dva[e, span(n), :] += dv

    def gather_all(e, dk, dv, first):
        for n in range(chunks):
            part = slice(wide // chunks * n, wide // chunks * (n + 1))
            gather(e, n, dk[part], dv[part], first)

    def totals(e, n):
        dk, dv = dka[e, span(n), :], dva[e, span(n), :]
        lane = lax.broadcasted_iota(jnp.int32, dv.shape, 1)
        dk = dk * scale
        return jnp.where(lane < NOPE, dk[:, :LANES], dv), dk[:, LANES:].T[:ROPE]

    def back_k(e, n):
        piece = pl.ds(n * chunk, chunk)
        return copy(kvs.at[e - 1, piece], kvr.at[e - 1, piece], s3k.at[e - 1, n], r3k.at[e - 1, n], at_x(e))

    def back_q(f):
        return copy(dqs.at[f - 1], dqr.at[f - 1], s3q.at[f - 1], r3q.at[f - 1], at_y(f))

    def send_k(e, n):
        kv, rot = totals(e, n)
        for c in range(chunk):
            kvs[e - 1, n * chunk + c, :T, :] = kv[T * c : T * (c + 1)].astype(KV_PART)
            kvs[e - 1, n * chunk + c, T:, :] = rot[:, T * c : T * (c + 1)].astype(KV_PART)
        back_k(e, n).start()

    prepare(0)
    dq, dk, dv = attend(whole_keys(0), 0)
    dqa[0] = dq
    gather_all(0, dk, dv, True)
    for e in range(1, GX):
        for d in order:
            relay_k(d, GX - e).wait_recv()
        dq, dk, dv = attend(whole_keys(e), 0)
        dqa[0] += dq
        gather_all(e, dk, dv, True)
    for f in range(1, GY):
        for d in order:
            relay_q(d, GY - f).wait_recv()
        prepare(f)
        for e in range(1, GX):
            for n in range(chunks):
                dq, dk, dv = attend(keys_at(e, n), f)
                if e == 1 and n == 0:
                    dqa[f] = dq
                else:
                    dqa[f] += dq
                gather(e, n, dk, dv, False)
                if f == GY - 1:
                    send_k(e, n)
        dq, dk, dv = attend(whole_keys(0), f)
        dqs[f - 1] = (dqa[f] + dq if GX > 1 else dq).astype(DQ_PART)
        back_q(f).start()
        gather_all(0, dk, dv, False)

    for d in far:
        first_l(d).wait_recv()
        repeat(1, TP, lambda i: hand_on(d, i).start())

    def home_k(d):
        to = partner(H, a, d, -1)
        return copy(kvo.at[order.index(d)], kvh.at[a], s4k.at[d - 1], r4k.at[d - 1], at_a(to))

    def home_r(d):
        to = partner(H, a, d, -1)
        return copy(ro.at[order.index(d)], rr.at[a], s4r.at[d - 1], r4r.at[d - 1], at_a(to))

    for d in far:
        repeat(1, TP, lambda i: hand_on(d, i).wait_recv())
    grads = []
    for n in range(chunks):
        for e in range(1, GX):
            back_k(e, n).wait_recv()
        kv, rot = totals(0, n)
        lats, finals = [], []
        for c in range(chunk):
            slot = n * chunk + c
            u = unit_of(slot, -1)
            part, turn = kv[T * c : T * (c + 1)], rot[:, T * c : T * (c + 1)]
            for e in range(1, GX):
                part = part + kvr[e - 1, slot, :T, :].astype(F32)
                turn = turn + kvr[e - 1, slot, T:, :].astype(F32)
            part = part.astype(BF16)
            kvo[slot] = part
            ro[slot] = turn
            lats.append(lb[u].reshape(T, lb.shape[3]))
            finals.append(part)
            if slot == 0:
                kvh[a] = part
                rr[a] = turn
            else:
                home_k(order[slot]).start()
        grads.append(dot(jnp.concatenate(lats, axis=0), jnp.concatenate(finals, axis=0), ((0,), (0,))))
    total = add_all(grads)
    rows = wgs.shape[1]
    wgs[...] = total.reshape(S, rows, LANES).astype(WG_PART)
    wgr[me] = wgs[me]

    def share(i):
        to = lax.rem(me + i, S)
        return copy(wgs.at[to], wgr.at[me], s5.at[i - 1], r5.at[i - 1], to)

    def spread(i, carry):
        share(i).start()
        return carry

    lax.fori_loop(1, S, spread, 0)
    for d in far:
        home_r(d).start()

    mine_q = dqa[0]
    for e in range(1, GY):
        back_q(e).wait_recv()
        mine_q = mine_q + dqr[e - 1].astype(F32)
    mine_q = (mine_q * scale).astype(BF16)
    for j in range(H):
        dqo[j] = mine_q[:, T * j : T * (j + 1)]

    def home_q(d):
        to = partner(H, a, d, 1)
        return copy(dqo.at[to], dqh.at[a], s4q.at[d - 1], r4q.at[d - 1], at_a(to))

    for d in far:
        home_q(d).start()
    dqh[a] = dqo[a]

    for d in far:
        home_k(d).wait_recv()
    for j in range(H):
        kg_ref[:, NOPE * j : NOPE * (j + 1)] = kvh[j, :, :NOPE]
        vg_ref[:, VDIM * j : VDIM * (j + 1)] = kvh[j, :, NOPE:]
    for d in far:
        home_r(d).wait_recv()
    rt[tpi] = add_all([rr[j] for j in range(H)])

    def swap(i):
        return copy_tp(rt.at[tpi], rt.at[tpi], s6.at[i - 1], r6.at[i - 1], i)

    repeat(1, TP, lambda i: swap(i).start())
    for d in far:
        home_q(d).wait_recv()
    qg_ref[...] = dqh[...].reshape(H * HEAD, T).astype(F32).T.astype(BF16)
    repeat(1, TP, lambda i: swap(i).wait_recv())
    rg_ref[...] = add_all([rt[i] for i in range(TP)])

    def arrive(i, carry):
        share(i).wait_recv()
        return carry

    lax.fori_loop(1, S, arrive, 0)
    for j in range(H):
        wg_ref[:, LANES * j : LANES * (j + 1)] = add_all([wgr[i * H + j].astype(F32) for i in range(G)])

    for d in far:
        for c in (first_q(d), first_k(d), first_l(d), home_k(d), home_r(d), home_q(d)):
            c.wait_send()
        repeat(1, TP, lambda i: hand_on(d, i).wait_send())
    for d in order:
        repeat(1, GY, lambda e: relay_q(d, e).wait_send())
        repeat(1, GX, lambda e: relay_k(d, e).wait_send())
    for n in range(chunks):
        repeat(1, GX, lambda e: back_k(e, n).wait_send())
    repeat(1, GY, lambda e: back_q(e).wait_send())
    repeat(1, TP, lambda i: swap(i).wait_send())

    def left(i, carry):
        share(i).wait_send()
        return carry

    lax.fori_loop(1, S, left, 0)


def one_stage_kernel(
    S, H, Z,
    q_in, lat_in, rot_in, w_in, log_in, out_in, go_in,
    qg_ref, kg_ref, vg_ref, rg_ref, wg_ref,
    q_ref, lat_ref, rot_ref, w_ref, log_ref, out_ref, go_ref, loads,
    qs, pk, wq, kb, lb, rp, key_ref, value_ref, turned_ref, dqa, dqx, dqr, dka, dva,
    kvo, kvh, ro, rr, rt, wgs, wgr, dqo, dqh,
    s1q, r1q, s1k, r1k, s2q, r2q, s3l, r3l, s4l, r4l, s5d, r5d,
    s6k, r6k, s6r, r6r, s6q, r6q, s7, r7, s8, r8,
):
    TP = 2
    NH = TP * H
    T = q_ref.shape[0]
    me = lax.axis_index("sp")
    c = lax.axis_index("tp")
    zh, g = me // NH, lax.rem(me, NH)
    k, p = g // H, lax.rem(g, H)
    straight = 1 - (c - k) * (c - k)
    scale = HEAD ** (-0.5)
    log2e = math.log2(math.e)
    far = distances(H)
    order = [0] + far
    quarter = T * ROPE // LANES
    wide = H * T

    barrier = pltpu.get_barrier_semaphore()

    def chip(z, kk, pp):
        return lax.rem(zh + z, Z) * NH + kk * H + pp

    def device(sp, tp):
        return {"sp": sp, "tp": tp}

    def copy(src, dst, ssem, rsem, where):
        return pltpu.make_async_remote_copy(
            src_ref=src, dst_ref=dst, send_sem=ssem, recv_sem=rsem,
            device_id=where, device_id_type=MESH,
        )

    def greet(where):
        pl.semaphore_signal(barrier, inc=1, device_id=where, device_id_type=MESH)

    sibling = device(me, 1 - c)

    pairs = (
        (q_in, q_ref), (go_in, go_ref), (out_in, out_ref), (log_in, log_ref),
        (lat_in, lat_ref), (w_in, w_ref), (rot_in, rot_ref),
    )
    fetch = [pltpu.make_async_copy(u, v, loads.at[i]) for i, (u, v) in enumerate(pairs)]
    for f in fetch:
        f.start()

    def at(d):
        return partner(H, p, d, 1)

    def unless_self(z, d, body):
        if z == 0 and d == 0:
            pl.when(straight == 0)(body)
        else:
            body()

    for z in range(Z - 1, -1, -1):
        for d in order:
            unless_self(z, d, lambda: greet(device(chip(z, c, at(d)), k)))
    for d in far:
        greet(device(chip(0, k, at(d)), c))
    greet(sibling)

    for f in fetch[:4]:
        f.wait()
    prod = out_ref[...].astype(F32) * go_ref[...].astype(F32)
    high = prod.astype(BF16)
    rest = (prod - high.astype(F32)).astype(BF16)
    head_of = lax.broadcasted_iota(jnp.int32, (8 * -(-H // 8), H * VDIM), 1) // VDIM
    picks = (head_of == lax.broadcasted_iota(jnp.int32, head_of.shape, 0)).astype(F32).astype(BF16)
    deltas = dot(picks, high, ((1,), (1,))) + dot(picks, rest, ((1,), (1,)))
    logs = log_ref[...] * log2e
    for j in range(H):
        start = HEAD * j
        qs[j, :T, :] = jnp.concatenate(
            [q_ref[:, start : start + NOPE], go_ref[:, VDIM * j : VDIM * (j + 1)]], axis=1)
        turned = q_ref[:, start + NOPE : start + HEAD]
        qs[j, T : T + quarter, :] = jnp.concatenate(
            [turned[quarter * i : quarter * (i + 1)] for i in range(LANES // ROPE)], axis=1)
        terms = three_terms(logs[j : j + 1]) + three_terms(deltas[j : j + 1])
        qs[j, T + quarter :, :] = jnp.concatenate(
            [t.astype(F32) for t in terms] + [jnp.zeros((STATS - 6, T), F32)], axis=0).astype(BF16)

    @pl.when(straight == 1)
    def _():
        wq[zh, c, p] = qs[p]

    pl.semaphore_wait(barrier, Z * H - straight + H - 1 + 1)

    def send_q(z, d):
        return copy(qs.at[at(d)], wq.at[zh, k, p], s1q.at[z, d], r1q.at[z, d], device(chip(z, c, at(d)), k))

    def take_q(z, d):
        place = wq.at[lax.rem(zh + z, Z), c, at(d)]
        return copy(place, place, s1q.at[z, d], r1q.at[(Z - z) % Z, d], sibling)

    def send_k(d):
        return copy(pk.at[at(d)], kb.at[p], s1k.at[d], r1k.at[d], device(chip(0, c, at(d)), k))

    def take_k(d):
        place = kb.at[at(d)]
        return copy(place, place, s1k.at[d], r1k.at[d], sibling)

    def pass_q(z, d):
        place = wq.at[lax.rem(zh + z, Z), c, at(d)]
        return copy(place, place, s2q.at[z, d], r2q.at[z, d], sibling)

    def passed_q(z, d):
        place = wq.at[lax.rem(zh + z, Z), 1 - c, at(d)]
        return copy(place, place, s2q.at[z, d], r2q.at[z, d], sibling)

    by_hops = far + [0]
    for d in by_hops:
        unless_self(0, d, lambda: send_q(0, d).start())
    for f in fetch[4:]:
        f.wait()
    joined = dot(lat_ref[...], w_ref[...], ((1,), (0,))).astype(BF16)
    for j in range(H):
        pk[j, :T, :] = joined[:, LANES * j : LANES * (j + 1)]
        pk[j, T:, :] = rot_ref[...]
    for d in by_hops:
        unless_self(0, d, lambda: send_k(d).start())
    for z in range(1, Z):
        for d in by_hops:
            send_q(z, d).start()

    @pl.when(straight == 1)
    def _():
        kb[p] = pk[p]
        lb[p] = lat_ref[...]

    def cross_l():
        return copy(lat_ref, lb.at[p], s3l, r3l, device(chip(0, c, p), k))

    pl.when(straight == 0)(lambda: cross_l().start())

    def take_all(z):
        for d in order:
            unless_self(z, d, lambda: take_q(z, d).wait_recv())
            pass_q(z, d).start()

    take_all(0)
    for d in order:
        unless_self(0, d, lambda: take_k(d).wait_recv())

    lane = lax.broadcasted_iota(jnp.int32, (T, LANES), 1)
    for j in range(H):
        kv = kb[j, :T, :]
        rot = kb[j, T:, :]
        part = jnp.where(lane < NOPE, kv, jnp.zeros_like(kv))
        column = rot.astype(F32).T.astype(BF16)
        key_ref[T * j : T * (j + 1), :LANES] = part
        key_ref[T * j : T * (j + 1), LANES:] = jnp.concatenate(
            [column, jnp.zeros((T, LANES - ROPE), BF16)], axis=1)
        value_ref[T * j : T * (j + 1), :] = kv - part
        turned_ref[:NOPE, T * j : T * (j + 1)] = kv.astype(F32).T.astype(BF16)[:NOPE]
        turned_ref[NOPE:, T * j : T * (j + 1)] = rot

    def attend(z, kk):
        zs = lax.rem(zh + z, Z)
        ks = lax.rem(c + kk, TP)
        for j in range(H):
            packed = wq[zs, ks, j, T : T + quarter, :]
            for i in range(LANES // ROPE):
                turn = packed if i == 0 else jnp.concatenate(
                    [packed[:, ROPE * i :], packed[:, : ROPE * i]], axis=1)
                rp[T * j + quarter * i : T * j + quarter * (i + 1), :] = turn
        row = wq[zs, ks, :, :T, :].reshape(wide, LANES)
        both = jnp.concatenate([row, rp[...]], axis=1)
        stats = [wq[zs, ks, j, T + quarter :, :].astype(F32) for j in range(H)]
        log = jnp.concatenate([t[0:1] + t[1:2] + t[2:3] for t in stats], axis=1)
        delta = jnp.concatenate([t[3:4] + t[4:5] + t[5:6] for t in stats], axis=1)
        s = dot(key_ref[...], both, ((1,), (1,)))
        dp = dot(value_ref[...], row, ((1,), (1,)))
        prob = jnp.exp2(s * (scale * log2e) - log)
        ds = (prob * (dp - delta)).astype(BF16)
        dq = dot(turned_ref[...], ds, ((1,), (0,)))
        dk = dot(ds, both, ((1,), (0,)))
        dv = dot(prob.astype(BF16), row, ((1,), (0,)))
        return dq, dk, dv

    def gather(z, kk):
        dq, dk, dv = attend(z, kk)
        if kk == 0:
            dqa[z] = dq
        else:
            dqx[z] = dq
            swap_d(z).start()
        if z == 0 and kk == 0:
            dka[...], dva[...] = dk, dv
        else:
            dka[...] += dk
            dva[...] += dv

    def swap_d(z):
        return copy(dqx.at[z], dqr.at[z], s5d.at[z], r5d.at[z], sibling)

    def home_q(z, d):
        return copy(dqo.at[z, at(d)], dqh.at[zh, p], s6q.at[z, d], r6q.at[z, d],
                    device(chip(z, c, at(d)), k))

    def home_took_q(z, d):
        place = dqh.at[lax.rem(zh + z, Z), at(d)]
        return copy(place, place, s6q.at[z, d], r6q.at[(Z - z) % Z, d], sibling)

    def finish_q(z):
        swap_d(z).wait_recv()
        total = ((dqa[z] + dqr[z]) * scale).astype(BF16)
        for j in range(H):
            dqo[z, j] = total[:, T * j : T * (j + 1)]
        for d in by_hops:
            unless_self(z, d, lambda: home_q(z, d).start())
        if z == 0:
            @pl.when(straight == 1)
            def _():
                dqh[zh, p] = dqo[0, p]

    def plane_l(d):
        return copy(lb.at[p], lb.at[p], s4l.at[d - 1], r4l.at[d - 1], device(chip(0, k, at(d)), c))

    def take_l(d):
        place = lb.at[at(d)]
        return copy(place, place, s4l.at[d - 1], r4l.at[d - 1], sibling)

    gather(0, 0)
    pl.when(straight == 0)(lambda: cross_l().wait_recv())
    for d in far:
        plane_l(d).start()
    for d in order:
        passed_q(0, d).wait_recv()
    gather(0, 1)
    for z in range(1, Z):
        take_all(z)
        if z == 1:
            finish_q(0)
        gather(z, 0)
        for d in order:
            passed_q(z, d).wait_recv()
        gather(z, 1)
    if Z == 1:
        finish_q(0)

    dk, dv = dka[...] * scale, dva[...]
    lane = lax.broadcasted_iota(jnp.int32, dv.shape, 1)
    kv = jnp.where(lane < NOPE, dk[:, :LANES], dv).astype(BF16)
    rot = dk[:, LANES:].T[:ROPE]
    for j in range(H):
        kvo[j] = kv[T * j : T * (j + 1)]
        ro[j] = rot[:, T * j : T * (j + 1)]

    def home_k(d):
        return copy(kvo.at[at(d)], kvh.at[p], s6k.at[d], r6k.at[d], device(chip(0, c, at(d)), k))

    def home_r(d):
        return copy(ro.at[at(d)], rr.at[p], s6r.at[d], r6r.at[d], device(chip(0, c, at(d)), k))

    def home_took_k(d):
        place = kvh.at[at(d)]
        return copy(place, place, s6k.at[d], r6k.at[d], sibling)

    def home_took_r(d):
        place = rr.at[at(d)]
        return copy(place, place, s6r.at[d], r6r.at[d], sibling)

    for d in by_hops:
        unless_self(0, d, lambda: home_k(d).start())

    for d in far:
        take_l(d).wait_recv()
    rows = wgs.shape[1]
    total = dot(lb[...].reshape(wide, lb.shape[2]), kv, ((0,), (0,)))
    wgs[...] = total.reshape(S, rows, LANES).astype(WG_PART)
    spread = [(z, kk, d) for z in range(Z - 1, -1, -1) for kk in (1, 0) for d in by_hops]

    def at_k(kk):
        return lax.rem(k + kk, TP)

    def share(z, kk, d):
        to = chip(z, at_k(kk), at(d))
        return copy(wgs.at[to], wgr.at[zh, c, p], s7.at[z, kk, d], r7.at[z, c, d], device(to, k))

    @pl.when(straight == 1)
    def _():
        kvh[p] = kvo[p]
        rr[p] = ro[p]
        wgr[zh, c, p] = wgs[me]

    def unless_own(z, kk, d, body):
        if kk == 0:
            unless_self(z, d, body)
        else:
            body()

    def take_share(z, kk, d):
        core = lax.rem(c + kk, TP)
        place = wgr.at[lax.rem(zh + z, Z), core, at(d)]
        return copy(place, place, s7.at[z, kk, d], r7.at[(Z - z) % Z, core, d], sibling)

    for z, kk, d in spread:
        unless_own(z, kk, d, lambda: share(z, kk, d).start())
    for z in range(1, Z):
        finish_q(z)
    for d in by_hops:
        unless_self(0, d, lambda: home_r(d).start())

    for d in order:
        unless_self(0, d, lambda: home_took_k(d).wait_recv())
    for j in range(H):
        kg_ref[:, NOPE * j : NOPE * (j + 1)] = kvh[j, :, :NOPE]
        vg_ref[:, VDIM * j : VDIM * (j + 1)] = kvh[j, :, NOPE:]
    for d in order:
        unless_self(0, d, lambda: home_took_r(d).wait_recv())
    rt[c] = add_all([rr[j] for j in range(H)])

    def swap():
        return copy(rt.at[c], rt.at[c], s8, r8, sibling)

    swap().start()
    for z in range(Z):
        for d in order:
            unless_self(z, d, lambda: home_took_q(z, d).wait_recv())
    summed = add_all([dqh[z].reshape(H * HEAD, T).astype(F32) for z in range(Z)])
    qg_ref[...] = summed.T.astype(BF16)
    pltpu.make_async_remote_copy(
        src_ref=rt.at[1 - c], dst_ref=rt.at[1 - c], send_sem=s8, recv_sem=r8,
        device_id=sibling, device_id_type=MESH).wait_recv()
    rg_ref[...] = add_all([rt[i] for i in range(TP)])
    for z, kk, d in spread:
        unless_own(z, kk, d, lambda: take_share(z, kk, d).wait_recv())
    for j in range(H):
        wg_ref[:, LANES * j : LANES * (j + 1)] = add_all(
            [wgr[z, i, j].astype(F32) for z in range(Z) for i in range(TP)])

    for z in range(Z):
        for d in order:
            unless_self(z, d, lambda: send_q(z, d).wait_send())
            unless_self(z, d, lambda: home_q(z, d).wait_send())
            pass_q(z, d).wait_send()
        swap_d(z).wait_send()
    for d in order:
        for what in (send_k, home_k, home_r):
            unless_self(0, d, lambda: what(d).wait_send())
    for d in far:
        plane_l(d).wait_send()
    pl.when(straight == 0)(lambda: cross_l().wait_send())
    for z, kk, d in spread:
        unless_own(z, kk, d, lambda: share(z, kk, d).wait_send())
    swap().wait_send()


def put_out(*refs):
    copies = [pltpu.make_async_copy(refs[i], refs[5 + i], refs[10].at[i]) for i in range(5)]
    for c in copies:
        c.start()
    for c in copies:
        c.wait()


def dma(*n):
    return pltpu.SemaphoreType.DMA(tuple(max(k, 1) for k in n))


def pairs(*n):
    return [dma(*n), dma(*n)]


def vm(shape, kind):
    return pltpu.VMEM(tuple(max(k, 1) for k in shape), kind)


def general_plan(S, TP, H, T, rank, arrays):
    G = S // H
    GX = max(d for d in range(1, math.isqrt(G) + 1) if G % d == 0)
    GY = G // GX
    rows = rank // S
    wide = H * T
    unit = T + T * ROPE // LANES + STATS
    return functools.partial(general_kernel, S, TP, H, GY, GX), [
        *[vm(u.shape, u.dtype) for u in arrays], dma(len(arrays)),
        vm((H, unit, LANES), BF16), vm((H, T + ROPE, LANES), BF16),
        vm((GY, H, unit, LANES), BF16), vm((GX, H, T + ROPE, LANES), BF16), vm((H, TP, T // TP, rank), BF16),
        vm((GY, wide, LANES), BF16), vm((GY, HEAD, wide), F32),
        *[vm((GY - 1, HEAD, wide), DQ_PART)] * 2, *[vm((GX - 1, H, T + ROPE, LANES), KV_PART)] * 2,
        vm((GX, wide, 2 * LANES), F32), vm((GX, wide, LANES), F32),
        *[vm((H, T, LANES), BF16)] * 2, *[vm((H, ROPE, T), F32)] * 2, vm((TP, ROPE, T), F32),
        *[vm((S, rows, LANES), WG_PART)] * 2, *[vm((H, HEAD, T), BF16)] * 2,
        *pairs(H - 1), *pairs(H - 1), *pairs(H - 1), *pairs(GY - 1, H), *pairs(GX - 1, H),
        *pairs(GY - 1), *pairs(GX - 1, H),
        *pairs(H - 1), *pairs(H - 1), *pairs(H - 1), *pairs(S - 1), *pairs(TP - 1), *pairs(H - 1, TP - 1),
    ]


def one_stage_plan(S, H, T, rank, arrays):
    Z = S // (2 * H)
    rows = rank // S
    wide = H * T
    unit = T + T * ROPE // LANES + STATS
    return functools.partial(one_stage_kernel, S, H, Z), [
        *[vm(u.shape, u.dtype) for u in arrays], dma(len(arrays)),
        vm((H, unit, LANES), BF16), vm((H, T + ROPE, LANES), BF16),
        vm((Z, 2, H, unit, LANES), BF16), vm((H, T + ROPE, LANES), BF16), vm((H, T, rank), BF16),
        vm((wide, LANES), BF16), vm((wide, 2 * LANES), BF16), vm((wide, LANES), BF16), vm((HEAD, wide), BF16),
        *[vm((Z, HEAD, wide), F32)] * 3, vm((wide, 2 * LANES), F32), vm((wide, LANES), F32),
        *[vm((H, T, LANES), BF16)] * 2, *[vm((H, ROPE, T), F32)] * 2, vm((2, ROPE, T), F32),
        vm((S, rows, LANES), WG_PART), vm((Z, 2, H, rows, LANES), WG_PART), *[vm((Z, H, HEAD, T), BF16)] * 2,
        *pairs(Z, H), *pairs(H), *pairs(Z, H), pltpu.SemaphoreType.DMA, pltpu.SemaphoreType.DMA, *pairs(H - 1),
        *pairs(Z), *pairs(H), *pairs(H), *pairs(Z, H), *pairs(Z, 2, H), pltpu.SemaphoreType.DMA, pltpu.SemaphoreType.DMA,
    ]


def per_device(S, TP, queries, latents, rot_key, kv_weight, log_sums, outputs, out_grad):
    T, rank = latents.shape
    H = log_sums.shape[1]
    rows = rank // S
    arrays = (queries, latents, rot_key.T, kv_weight, log_sums.T, outputs, out_grad)
    if TP == 2 and H > 1 and power_of_two(H) and S % (TP * H) == 0:
        body, scratch = one_stage_plan(S, H, T, rank, arrays)
    else:
        body, scratch = general_plan(S, TP, H, T, rank, arrays)
    shapes = [
        ((T, H * HEAD), BF16), ((T, H * NOPE), BF16), ((T, H * VDIM), BF16),
        ((ROPE, T), F32), ((rows, H * LANES), F32),
    ]
    held = sum(u[0] * -(-u[1] // LANES) * LANES * jnp.dtype(t).itemsize for u, t in shapes)
    results = pl.pallas_call(
        body,
        out_shape=[pltpu.VMEM(*u) for u in shapes],
        in_specs=[pl.BlockSpec(memory_space=pltpu.HBM)] * 7,
        out_specs=[pl.BlockSpec(memory_space=pltpu.VMEM)] * 5,
        scratch_shapes=scratch,
        compiler_params=pltpu.CompilerParams(
            collective_id=0, has_side_effects=True, vmem_limit_bytes=VMEM_BYTES - held - SPARE
        ),
    )(*arrays)
    query_grad, key_grad, value_grad, rot_grad, weight_grad = pl.pallas_call(
        put_out,
        out_shape=[jax.ShapeDtypeStruct(*u) for u in shapes],
        in_specs=[pl.BlockSpec(memory_space=pltpu.VMEM)] * 5,
        out_specs=[pl.BlockSpec(memory_space=pltpu.HBM)] * 5,
        scratch_shapes=[dma(5)],
        compiler_params=pltpu.CompilerParams(vmem_limit_bytes=1 << 20),
    )(*results)
    return query_grad, key_grad, value_grad, rot_grad.T, weight_grad


def solution(mesh):
    placed = (
        P("sp", "tp"), P("sp", None), P("sp", None), P(None, "tp"),
        P("sp", "tp"), P("sp", "tp"), P("sp", "tp"),
    )
    return jax.shard_map(
        functools.partial(per_device, mesh.shape["sp"], mesh.shape["tp"]),
        mesh=mesh,
        in_specs=placed,
        out_specs=(P("sp", "tp"), P("sp", "tp"), P("sp", "tp"), P("sp", None), P("sp", "tp")),
        check_vma=False,
    )
```

```python
import functools
import math

import jax
import jax.numpy as jnp
from jax import lax
from jax.experimental import pallas as pl
from jax.experimental.pallas import tpu as pltpu
from jax.sharding import PartitionSpec as P

NOPE = 64
ROPE = 32
VDIM = 64
HEAD = NOPE + ROPE
LANES = 128
STATS = 8
VMEM_BYTES = 67043328
SPARE = 8192
MESH = pl.DeviceIdType.MESH
F32 = jnp.float32
BF16 = jnp.bfloat16
KV_PART = BF16
DQ_PART = BF16
WG_PART = BF16


def dot(x, y, dims):
    return lax.dot_general(x, y, (dims, ((), ())), preferred_element_type=F32)


def three_terms(x):
    hi = x.astype(BF16)
    rest = x - hi.astype(F32)
    mid = rest.astype(BF16)
    low = (rest - mid.astype(F32)).astype(BF16)
    return hi, mid, low


def repeat(start, stop, body):
    if stop - start <= 4:
        for i in range(start, stop):
            body(i)
    else:
        def step(i, carry):
            body(i)
            return carry

        lax.fori_loop(start, stop, step, 0)


def add_all(terms):
    return functools.reduce(lambda x, y: x + y, terms)


def power_of_two(n):
    return n & (n - 1) == 0


def partner(n, i, d, sign):
    if not power_of_two(n):
        return lax.rem(i + sign * d + n, n)
    bit = 1
    result = i
    while bit <= d:
        if d & bit:
            result = result + bit * (1 - 2 * lax.rem(i // bit, 2))
        bit *= 2
    return result


def distances(n):
    if not power_of_two(n):
        return list(range(1, n))
    return sorted(range(1, n), key=lambda d: -bin(d).count("1"))


def kernel(
    S, TP, H, GY, GX,
    q_in, lat_in, rot_in, w_in, log_in, out_in, go_in,
    qg_ref, kg_ref, vg_ref, rg_ref, wg_ref,
    q_ref, lat_ref, rot_ref, w_ref, log_ref, out_ref, go_ref, loads,
    qs, pk, wq, kb, rk, lb, rp, key_ref, value_ref, turned_ref, dqa, dqs, dqr, kvs, kvr, rps, rpr, dka, dva,
    kvo, kvh, ro, rr, rt, wgs, wgr, dqo, dqh,
    s1q, r1q, s1k, r1k, s1l, r1l, s2q, r2q, s2k, r2k, s3q, r3q, s3k, r3k,
    s4q, r4q, s4k, r4k, s4r, r4r, s5, r5, s6, r6, s8, r8,
    s9a, r9a, s9x, r9x, s9t, r9t, s9b, r9b,
):
    G = GY * GX
    T = q_ref.shape[0]
    me = lax.axis_index("sp")
    tpi = lax.axis_index("tp")
    a, b = lax.rem(me, H), me // H
    y, x = b // GX, lax.rem(b, GX)
    scale = HEAD ** (-0.5)
    log2e = math.log2(math.e)
    far = distances(H)
    quarter = T * ROPE // LANES

    barrier = pltpu.get_barrier_semaphore()

    def greet(to):
        pl.semaphore_signal(barrier, inc=1, device_id={"sp": to}, device_id_type=MESH)

    def greet_tp(i):
        pl.semaphore_signal(barrier, inc=1, device_id={"tp": lax.rem(tpi + i, TP)}, device_id_type=MESH)

    def at_a(z):
        return b * H + z

    def at_y(e):
        return (lax.rem(y + e, GY) * GX + x) * H + a

    def at_x(e):
        return (y * GX + lax.rem(x + e, GX)) * H + a

    pairs = (
        (q_in, q_ref), (go_in, go_ref), (out_in, out_ref), (log_in, log_ref),
        (lat_in, lat_ref), (w_in, w_ref), (rot_in, rot_ref),
    )
    fetch = [pltpu.make_async_copy(u, v, loads.at[i]) for i, (u, v) in enumerate(pairs)]
    for f in fetch:
        f.start()
    for d in far:
        greet(at_a(partner(H, a, d, 1)))
    repeat(1, GY, lambda e: greet(at_y(e)))
    repeat(1, GX, lambda e: greet(at_x(e)))
    repeat(1, TP, greet_tp)

    def copy(src, dst, ssem, rsem, sp):
        return pltpu.make_async_remote_copy(
            src_ref=src, dst_ref=dst, send_sem=ssem, recv_sem=rsem,
            device_id={"sp": sp}, device_id_type=MESH,
        )

    def copy_tp(src, dst, ssem, rsem, i):
        return pltpu.make_async_remote_copy(
            src_ref=src, dst_ref=dst, send_sem=ssem, recv_sem=rsem,
            device_id={"tp": lax.rem(tpi + i, TP)}, device_id_type=MESH,
        )

    for f in fetch[:4]:
        f.wait()
    prod = out_ref[...].astype(F32) * go_ref[...].astype(F32)
    high = prod.astype(BF16)
    rest = (prod - high.astype(F32)).astype(BF16)
    head_of = lax.broadcasted_iota(jnp.int32, (8 * -(-H // 8), H * VDIM), 1) // VDIM
    picks = (head_of == lax.broadcasted_iota(jnp.int32, head_of.shape, 0)).astype(F32).astype(BF16)
    deltas = dot(picks, high, ((1,), (1,))) + dot(picks, rest, ((1,), (1,)))
    logs = log_ref[...] * log2e
    for j in range(H):
        start = HEAD * j
        qs[j, :T, :] = jnp.concatenate(
            [q_ref[:, start : start + NOPE], go_ref[:, VDIM * j : VDIM * (j + 1)]], axis=1)
        turned = q_ref[:, start + NOPE : start + HEAD]
        qs[j, T : T + quarter, :] = jnp.concatenate(
            [turned[quarter * i : quarter * (i + 1)] for i in range(LANES // ROPE)], axis=1)
        terms = three_terms(logs[j : j + 1]) + three_terms(deltas[j : j + 1])
        qs[j, T + quarter :, :] = jnp.concatenate(
            [t.astype(F32) for t in terms] + [jnp.zeros((STATS - 6, T), F32)], axis=0).astype(BF16)
    wq[y, a] = qs[a]
    pl.semaphore_wait(barrier, H - 1 + GY - 1 + GX - 1 + TP - 1)

    def first_q(d):
        to = partner(H, a, d, 1)
        return copy(qs.at[to], wq.at[y, a], s1q.at[d - 1], r1q.at[d - 1], at_a(to))

    def first_k(d):
        to = partner(H, a, d, 1)
        return copy(pk.at[to], kb.at[x, a], s1k.at[d - 1], r1k.at[d - 1], at_a(to))

    def first_r(d):
        return copy(rot_ref, rk.at[x, a], s9a.at[d - 1], r9a.at[d - 1], at_a(partner(H, a, d, 1)))

    def relay_r(d, e):
        src = rk.at[x, partner(H, a, d, -1)]
        return copy(src, src, s9x.at[e - 1, d], r9x.at[e - 1, d], at_x(e))

    def over_r(d, e):
        src = rk.at[lax.rem(x + e, GX), partner(H, a, d, -1)]
        return pltpu.make_async_remote_copy(
            src_ref=src, dst_ref=src, send_sem=s9t.at[e, d], recv_sem=r9t.at[e, d],
            device_id={"tp": tpi + 1 - 2 * lax.rem(tpi, 2)}, device_id_type=MESH,
        )

    def leading(body):
        if TP % 2:
            body()
        else:
            pl.when(lax.rem(tpi, 2) == 1)(body)

    def hand_over(d, e):
        if TP % 2 == 0:
            over_r(d, e).start()

    def relay_q(d, e):
        src = wq.at[y, partner(H, a, d, -1)]
        return copy(src, src, s2q.at[e - 1, d], r2q.at[e - 1, d], at_y(e))

    def relay_k(d, e):
        src = kb.at[x, partner(H, a, d, -1)]
        return copy(src, src, s2k.at[e - 1, d], r2k.at[e - 1, d], at_x(e))

    for d in far:
        first_q(d).start()
    repeat(1, GY, lambda e: relay_q(0, e).start())
    for f in fetch[4:]:
        f.wait()
    joined = dot(lat_ref[...], w_ref[...], ((1,), (0,))).astype(BF16)
    for j in range(H):
        pk[j] = joined[:, LANES * j : LANES * (j + 1)]
    kb[x, a] = pk[a]
    rk[x, a] = rot_ref[...]
    for d in far:
        first_k(d).start()
    repeat(1, GX, lambda e: relay_k(0, e).start())

    @leading
    def _():
        for d in far:
            first_r(d).start()
        for e in range(1, GX):
            relay_r(0, e).start()

    lb[a] = lat_ref[...].reshape(lb.shape[1:])
    for d in far:
        first_q(d).wait_recv()
        repeat(1, GY, lambda e: relay_q(d, e).start())
    for d in far:
        first_k(d).wait_recv()
        repeat(1, GX, lambda e: relay_k(d, e).start())

    @leading
    def _():
        for d in far:
            first_r(d).wait_recv()
            for e in range(1, GX):
                relay_r(d, e).start()
            hand_over(d, 0)

    slab = T // TP
    mine = lat_ref.at[pl.ds(pl.multiple_of(tpi * slab, slab), slab)]

    def first_l(d):
        return copy(mine, lb.at[a, tpi], s1l.at[d - 1], r1l.at[d - 1], at_a(partner(H, a, d, 1)))

    def hand_on(d, i):
        piece = lb.at[partner(H, a, d, -1), tpi]
        return copy_tp(piece, piece, s8.at[d - 1, i - 1], r8.at[d - 1, i - 1], i)

    wide = H * T
    order = [0] + far
    chunks = 2 if H % 2 == 0 else H
    chunk = H // chunks
    some = chunk * T

    def unit_of(n, c):
        return partner(H, a, order[n * chunk + c], -1)

    def part_of(n):
        return order[n * chunk : (n + 1) * chunk]

    def prepare_keys(e, n):
        where = lax.rem(x + e, GX)
        lane = lax.broadcasted_iota(jnp.int32, (T, LANES), 1)
        for c in range(chunk):
            rows = slice(T * c, T * (c + 1))
            kv = kb[where, unit_of(n, c)]
            rot = rk[where, unit_of(n, c)]
            part = jnp.where(lane < NOPE, kv, jnp.zeros_like(kv))
            column = rot.astype(F32).T.astype(BF16)
            key_ref[e, n, rows, :LANES] = part
            key_ref[e, n, rows, LANES:] = jnp.concatenate([column, jnp.zeros((T, LANES - ROPE), BF16)], axis=1)
            value_ref[e, n, rows, :] = kv - part
            turned_ref[e, n, :NOPE, rows] = kv.astype(F32).T.astype(BF16)[:NOPE]
            turned_ref[e, n, NOPE:, rows] = rot

    def prepare_queries(f, n):
        col = lax.rem(y + f, GY)
        for c in range(chunk):
            packed = wq[col, unit_of(n, c), T : T + quarter, :]
            for m in range(LANES // ROPE):
                part = packed if m == 0 else jnp.concatenate(
                    [packed[:, ROPE * m :], packed[:, : ROPE * m]], axis=1)
                rp[f, n, T * c + quarter * m : T * c + quarter * (m + 1), :] = part

    begun = set()

    def attend(keys, queries):
        key = jnp.concatenate([key_ref[e, n] for e, n in keys], axis=0)
        value = jnp.concatenate([value_ref[e, n] for e, n in keys], axis=0)
        turned = jnp.concatenate([turned_ref[e, n] for e, n in keys], axis=1)
        rows, logs, deltas = [], [], []
        for f, n in queries:
            col = lax.rem(y + f, GY)
            for c in range(chunk):
                rows.append(wq[col, unit_of(n, c), :T, :])
                t = wq[col, unit_of(n, c), T + quarter :, :].astype(F32)
                logs.append(t[0:1] + t[1:2] + t[2:3])
                deltas.append(t[3:4] + t[4:5] + t[5:6])
        row = jnp.concatenate(rows, axis=0)
        both = jnp.concatenate([row, jnp.concatenate([rp[f, n] for f, n in queries], axis=0)], axis=1)
        log, delta = jnp.concatenate(logs, axis=1), jnp.concatenate(deltas, axis=1)
        s = dot(key, both, ((1,), (1,)))
        dp = dot(value, row, ((1,), (1,)))
        p = jnp.exp2(s * (scale * log2e) - log)
        ds = (p * (dp - delta)).astype(BF16)
        dq = dot(turned, ds, ((1,), (0,)))
        dk = dot(ds, both, ((1,), (0,)))
        dv = dot(p.astype(BF16), row, ((1,), (0,)))
        for i, (f, n) in enumerate(queries):
            piece = dq[:, some * i : some * (i + 1)]
            dqa[f, n] = dqa[f, n] + piece if ("q", f, n) in begun else piece
            begun.add(("q", f, n))
        for i, (e, n) in enumerate(keys):
            span = slice(some * i, some * (i + 1))
            if ("k", e, n) in begun:
                dka[e, n] += dk[span]
                dva[e, n] += dv[span]
            else:
                dka[e, n], dva[e, n] = dk[span], dv[span]
            begun.add(("k", e, n))

    def pair(e, n):
        dk, dv = dka[e, n, :, :LANES], dva[e, n]
        lane = lax.broadcasted_iota(jnp.int32, dv.shape, 1)
        return jnp.where(lane < NOPE, dk * scale, dv)

    def turned_part(e):
        return (jnp.concatenate([dka[e, n, :, LANES:] for n in range(chunks)], axis=0) * scale).T[:ROPE]

    def back_k(e, n):
        piece = pl.ds(n * chunk, chunk)
        return copy(kvs.at[e - 1, piece], kvr.at[e - 1, piece], s3k.at[e - 1, n], r3k.at[e - 1, n], at_x(e))

    def back_q(f, n):
        return copy(dqs.at[f - 1, n], dqr.at[f - 1, n], s3q.at[f - 1, n], r3q.at[f - 1, n], at_y(f))

    def back_r(e):
        return copy(rps.at[e - 1], rpr.at[e - 1], s9b.at[e - 1], r9b.at[e - 1], at_x(e))

    def send_k(e, n):
        kv = pair(e, n)
        for c in range(chunk):
            kvs[e - 1, n * chunk + c] = kv[T * c : T * (c + 1)].astype(KV_PART)
        back_k(e, n).start()

    def take_over(e, ds):
        if TP % 2 == 0:
            @pl.when(lax.rem(tpi, 2) == 0)
            def _():
                for d in ds:
                    over_r(d, e).wait_recv()

    def following(body):
        if TP % 2:
            body()
        else:
            pl.when(lax.rem(tpi, 2) == 0)(body)

    take_over(0, far)
    keys, queries = [], []
    for n in range(chunks):
        prepare_keys(0, n)
        prepare_queries(0, n)
        keys.append((0, n))
        queries.append((0, n))
    attend(keys, queries)
    for d in far:
        first_l(d).start()

    def new_keys(e, n):
        for d in part_of(n):
            relay_k(d, GX - e).wait_recv()

        @leading
        def _():
            for d in part_of(n):
                relay_r(d, GX - e).wait_recv()
                hand_over(d, e)

        take_over(e, part_of(n))
        prepare_keys(e, n)
        attend([(e, n)], queries)
        keys.append((e, n))

    def latents_on():
        for d in far:
            first_l(d).wait_recv()
            repeat(1, TP, lambda i: hand_on(d, i).start())

    def close_queries(f, n):
        dqs[f - 1, n] = dqa[f, n].astype(DQ_PART)
        following(lambda: back_q(f, n).start())

    def new_queries(f, n, last):
        for d in part_of(n):
            relay_q(d, GY - f).wait_recv()
        prepare_queries(f, n)
        if last:
            others = [i for i in keys if i[0] > 0]
            if others:
                attend(others, [(f, n)])
                for i in others:
                    send_k(*i)
            attend([i for i in keys if i[0] == 0], [(f, n)])
        else:
            attend(keys, [(f, n)])
        queries.append((f, n))

    more_keys = [(e, n) for e in range(1, GX) for n in range(chunks)]
    more_queries = [(f, n) for f in range(1, GY) for n in range(chunks)]
    lat_due = True
    while more_keys or more_queries:
        if more_keys:
            new_keys(*more_keys.pop(0))
            if not more_keys:
                for i in queries:
                    if i[0] > 0:
                        close_queries(*i)
        if lat_due and len(more_queries) <= 1:
            latents_on()
            lat_due = False
        if more_queries:
            i = more_queries.pop(0)
            new_queries(*i, last=not more_keys and not more_queries)
            if not more_keys:
                close_queries(*i)
    if lat_due:
        latents_on()
    if GY == 1:
        for e in range(1, GX):
            for n in range(chunks):
                send_k(e, n)
    for e in range(1, GX):
        rps[e - 1] = turned_part(e).astype(KV_PART)
        back_r(e).start()

    def home_k(d):
        to = partner(H, a, d, -1)
        return copy(kvo.at[order.index(d)], kvh.at[a], s4k.at[d - 1], r4k.at[d - 1], at_a(to))

    def home_r(d):
        to = partner(H, a, d, -1)
        return copy(ro.at[order.index(d)], rr.at[a], s4r.at[d - 1], r4r.at[d - 1], at_a(to))

    for d in far:
        repeat(1, TP, lambda i: hand_on(d, i).wait_recv())
    grads = []
    for n in range(chunks):
        for e in range(1, GX):
            back_k(e, n).wait_recv()
        kv = pair(0, n)
        lats, finals = [], []
        for c in range(chunk):
            slot = n * chunk + c
            part = kv[T * c : T * (c + 1)]
            for e in range(1, GX):
                part = part + kvr[e - 1, slot].astype(F32)
            part = part.astype(BF16)
            kvo[slot] = part
            lats.append(lb[unit_of(n, c)].reshape(T, lb.shape[3]))
            finals.append(part)
            if slot == 0:
                kvh[a] = part
            else:
                home_k(order[slot]).start()
        grads.append(dot(jnp.concatenate(lats, axis=0), jnp.concatenate(finals, axis=0), ((0,), (0,))))
    total = add_all(grads)
    rows = wgs.shape[1]
    wgs[...] = total.reshape(S, rows, LANES).astype(WG_PART)
    wgr[me] = wgs[me]

    spread = distances(S)

    def share(i):
        to = partner(S, me, i, 1)
        return copy(wgs.at[to], wgr.at[me], s5.at[i - 1], r5.at[i - 1], to)

    for i in spread:
        share(i).start()
    @leading
    def _():
        if TP % 2 == 0:
            for f in range(1, GY):
                for n in range(chunks):
                    back_q(f, n).start()

    turned = turned_part(0)
    for e in range(1, GX):
        back_r(e).wait_recv()
        turned = turned + rpr[e - 1].astype(F32)
    for slot in range(H):
        ro[slot] = turned[:, T * slot : T * (slot + 1)]
    rr[a] = ro[0]
    for d in far:
        home_r(d).start()

    def home_q(d):
        to = partner(H, a, d, -1)
        return copy(dqo.at[order.index(d)], dqh.at[a], s4q.at[d - 1], r4q.at[d - 1], at_a(to))

    for n in range(chunks):
        mine_q = dqa[0, n]
        for f in range(1, GY):
            back_q(f, n).wait_recv()
            mine_q = mine_q + dqr[f - 1, n].astype(F32)
        mine_q = (mine_q * scale).astype(BF16)
        for c, d in enumerate(part_of(n)):
            dqo[n * chunk + c] = mine_q[:, T * c : T * (c + 1)]
            if d == 0:
                dqh[a] = dqo[0]
            else:
                home_q(d).start()

    for d in far:
        home_k(d).wait_recv()
    for j in range(H):
        kg_ref[:, NOPE * j : NOPE * (j + 1)] = kvh[j, :, :NOPE]
        vg_ref[:, VDIM * j : VDIM * (j + 1)] = kvh[j, :, NOPE:]
    for d in far:
        home_r(d).wait_recv()
    rt[tpi] = add_all([rr[j] for j in range(H)])

    def swap(i):
        return copy_tp(rt.at[tpi], rt.at[tpi], s6.at[i - 1], r6.at[i - 1], i)

    repeat(1, TP, lambda i: swap(i).start())
    for d in far:
        home_q(d).wait_recv()
    qg_ref[...] = dqh[...].reshape(H * HEAD, T).astype(F32).T.astype(BF16)
    repeat(1, TP, lambda i: swap(i).wait_recv())
    rg_ref[...] = add_all([rt[i] for i in range(TP)])

    for i in spread:
        share(i).wait_recv()
    for j in range(H):
        wg_ref[:, LANES * j : LANES * (j + 1)] = add_all([wgr[i * H + j].astype(F32) for i in range(G)])

    for d in far:
        for c in (first_q(d), first_k(d), first_l(d), home_k(d), home_r(d), home_q(d)):
            c.wait_send()
        repeat(1, TP, lambda i: hand_on(d, i).wait_send())
    for d in order:
        repeat(1, GY, lambda e: relay_q(d, e).wait_send())
        repeat(1, GX, lambda e: relay_k(d, e).wait_send())
    for n in range(chunks):
        repeat(1, GX, lambda e: back_k(e, n).wait_send())
    for f in range(1, GY):
        for n in range(chunks):
            back_q(f, n).wait_send()
    repeat(1, TP, lambda i: swap(i).wait_send())
    for i in spread:
        share(i).wait_send()

    @leading
    def _():
        for d in far:
            first_r(d).wait_send()
        for e in range(1, GX):
            for d in order:
                relay_r(d, e).wait_send()
        if TP % 2 == 0:
            for d in far:
                over_r(d, 0).wait_send()
            for e in range(1, GX):
                for d in order:
                    over_r(d, e).wait_send()

    for e in range(1, GX):
        back_r(e).wait_send()


def put_out(*refs):
    copies = [pltpu.make_async_copy(refs[i], refs[5 + i], refs[10].at[i]) for i in range(5)]
    for c in copies:
        c.start()
    for c in copies:
        c.wait()


def per_device(S, TP, queries, latents, rot_key, kv_weight, log_sums, outputs, out_grad):
    T, rank = latents.shape
    H = log_sums.shape[1]
    G = S // H
    GX = max(d for d in range(1, math.isqrt(G) + 1) if G % d == 0)
    GY = G // GX
    rows = rank // S
    wide = H * T
    dma = lambda *n: pltpu.SemaphoreType.DMA(tuple(max(k, 1) for k in n))
    pairs = lambda *n: [dma(*n), dma(*n)]
    vm = lambda shape, kind: pltpu.VMEM(tuple(max(k, 1) for k in shape), kind)
    unit = T + T * ROPE // LANES + STATS
    chunks = 2 if H % 2 == 0 else H
    some = wide // chunks
    arrays = (queries, latents, rot_key.T, kv_weight, log_sums.T, outputs, out_grad)
    scratch = [
        *[vm(u.shape, u.dtype) for u in arrays], dma(len(arrays)),
        vm((H, unit, LANES), BF16), vm((H, T, LANES), BF16),
        vm((GY, H, unit, LANES), BF16), vm((GX, H, T, LANES), BF16), vm((GX, H, ROPE, T), BF16), vm((H, TP, T // TP, rank), BF16),
        vm((GY, chunks, some, LANES), BF16), vm((GX, chunks, some, 2 * LANES), BF16),
        vm((GX, chunks, some, LANES), BF16), vm((GX, chunks, HEAD, some), BF16), vm((GY, chunks, HEAD, some), F32),
        *[vm((GY - 1, chunks, HEAD, some), DQ_PART)] * 2, *[vm((GX - 1, H, T, LANES), KV_PART)] * 2, *[vm((GX - 1, ROPE, wide), KV_PART)] * 2,
        vm((GX, chunks, some, 2 * LANES), F32), vm((GX, chunks, some, LANES), F32),
        *[vm((H, T, LANES), BF16)] * 2, *[vm((H, ROPE, T), F32)] * 2, vm((TP, ROPE, T), F32),
        *[vm((S, rows, LANES), WG_PART)] * 2, *[vm((H, HEAD, T), BF16)] * 2,
        *pairs(H - 1), *pairs(H - 1), *pairs(H - 1), *pairs(GY - 1, H), *pairs(GX - 1, H),
        *pairs(GY - 1, chunks), *pairs(GX - 1, chunks),
        *pairs(H - 1), *pairs(H - 1), *pairs(H - 1), *pairs(S - 1), *pairs(TP - 1), *pairs(H - 1, TP - 1),
        *pairs(H - 1), *pairs(GX - 1, H), *pairs(GX, H), *pairs(GX - 1),
    ]
    shapes = [
        ((T, H * HEAD), BF16), ((T, H * NOPE), BF16), ((T, H * VDIM), BF16),
        ((ROPE, T), F32), ((rows, H * LANES), F32),
    ]
    held = sum(u[0] * -(-u[1] // LANES) * LANES * jnp.dtype(t).itemsize for u, t in shapes)
    results = pl.pallas_call(
        functools.partial(kernel, S, TP, H, GY, GX),
        out_shape=[pltpu.VMEM(*u) for u in shapes],
        in_specs=[pl.BlockSpec(memory_space=pltpu.HBM)] * 7,
        out_specs=[pl.BlockSpec(memory_space=pltpu.VMEM)] * 5,
        scratch_shapes=scratch,
        compiler_params=pltpu.CompilerParams(
            collective_id=0, has_side_effects=True, vmem_limit_bytes=VMEM_BYTES - held - SPARE
        ),
    )(*arrays)
    query_grad, key_grad, value_grad, rot_grad, weight_grad = pl.pallas_call(
        put_out,
        out_shape=[jax.ShapeDtypeStruct(*u) for u in shapes],
        in_specs=[pl.BlockSpec(memory_space=pltpu.VMEM)] * 5,
        out_specs=[pl.BlockSpec(memory_space=pltpu.HBM)] * 5,
        scratch_shapes=[dma(5)],
        compiler_params=pltpu.CompilerParams(vmem_limit_bytes=1 << 20),
    )(*results)
    return query_grad, key_grad, value_grad, rot_grad.T, weight_grad


def solution(mesh):
    placed = (
        P("sp", "tp"), P("sp", None), P("sp", None), P(None, "tp"),
        P("sp", "tp"), P("sp", "tp"), P("sp", "tp"),
    )
    return jax.shard_map(
        functools.partial(per_device, mesh.shape["sp"], mesh.shape["tp"]),
        mesh=mesh,
        in_specs=placed,
        out_specs=(P("sp", "tp"), P("sp", "tp"), P("sp", "tp"), P("sp", None), P("sp", "tp")),
        check_vma=False,
    )
```

```python
import functools
import math

import jax
import jax.numpy as jnp
from jax import lax
from jax.experimental import pallas as pl
from jax.experimental.pallas import tpu as pltpu
from jax.sharding import PartitionSpec as P

NOPE = 64
ROPE = 32
VDIM = 64
HEAD = NOPE + ROPE
LANES = 128
STATS = 8
VMEM_BYTES = 67043328
SPARE = 8192
MESH = pl.DeviceIdType.MESH
F32 = jnp.float32
BF16 = jnp.bfloat16
KV_PART = BF16
DQ_PART = BF16
WG_PART = BF16


def dot(x, y, dims):
    return lax.dot_general(x, y, (dims, ((), ())), preferred_element_type=F32)


def three_terms(x):
    hi = x.astype(BF16)
    rest = x - hi.astype(F32)
    mid = rest.astype(BF16)
    low = (rest - mid.astype(F32)).astype(BF16)
    return hi, mid, low


def repeat(start, stop, body):
    if stop - start <= 4:
        for i in range(start, stop):
            body(i)
    else:
        def step(i, carry):
            body(i)
            return carry

        lax.fori_loop(start, stop, step, 0)


def add_all(terms):
    return functools.reduce(lambda x, y: x + y, terms)


def power_of_two(n):
    return n & (n - 1) == 0


def partner(n, i, d, sign):
    if not power_of_two(n):
        return lax.rem(i + sign * d + n, n)
    bit = 1
    result = i
    while bit <= d:
        if d & bit:
            result = result + bit * (1 - 2 * lax.rem(i // bit, 2))
        bit *= 2
    return result


def distances(n):
    if not power_of_two(n):
        return list(range(1, n))
    return sorted(range(1, n), key=lambda d: -bin(d).count("1"))


def kernel(
    S, TP, H, GY, GX,
    q_in, lat_in, rot_in, w_in, log_in, out_in, go_in,
    qg_ref, kg_ref, vg_ref, rg_ref, wg_ref,
    q_ref, lat_ref, rot_ref, w_ref, log_ref, out_ref, go_ref, loads,
    qs, pk, wq, kb, rk, lb, rp, dqa, dqs, dqr, kvs, kvr, rps, rpr, dka, dva,
    kvo, kvh, ro, rr, rt, wgs, wgr, dqo, dqh,
    s1q, r1q, s1k, r1k, s1l, r1l, s2q, r2q, s2k, r2k, s3q, r3q, s3k, r3k,
    s4q, r4q, s4k, r4k, s4r, r4r, s5, r5, s6, r6, s8, r8,
    s9a, r9a, s9x, r9x, s9t, r9t, s9b, r9b,
):
    G = GY * GX
    T = q_ref.shape[0]
    me = lax.axis_index("sp")
    tpi = lax.axis_index("tp")
    a, b = lax.rem(me, H), me // H
    y, x = b // GX, lax.rem(b, GX)
    scale = HEAD ** (-0.5)
    log2e = math.log2(math.e)
    far = distances(H)
    quarter = T * ROPE // LANES

    barrier = pltpu.get_barrier_semaphore()

    def greet(to):
        pl.semaphore_signal(barrier, inc=1, device_id={"sp": to}, device_id_type=MESH)

    def greet_tp(i):
        pl.semaphore_signal(barrier, inc=1, device_id={"tp": lax.rem(tpi + i, TP)}, device_id_type=MESH)

    def at_a(z):
        return b * H + z

    def at_y(e):
        return (lax.rem(y + e, GY) * GX + x) * H + a

    def at_x(e):
        return (y * GX + lax.rem(x + e, GX)) * H + a

    pairs = (
        (q_in, q_ref), (go_in, go_ref), (out_in, out_ref), (log_in, log_ref),
        (lat_in, lat_ref), (w_in, w_ref), (rot_in, rot_ref),
    )
    fetch = [pltpu.make_async_copy(u, v, loads.at[i]) for i, (u, v) in enumerate(pairs)]
    for f in fetch:
        f.start()
    for d in far:
        greet(at_a(partner(H, a, d, 1)))
    repeat(1, GY, lambda e: greet(at_y(e)))
    repeat(1, GX, lambda e: greet(at_x(e)))
    repeat(1, TP, greet_tp)

    def copy(src, dst, ssem, rsem, sp):
        return pltpu.make_async_remote_copy(
            src_ref=src, dst_ref=dst, send_sem=ssem, recv_sem=rsem,
            device_id={"sp": sp}, device_id_type=MESH,
        )

    def copy_tp(src, dst, ssem, rsem, i):
        return pltpu.make_async_remote_copy(
            src_ref=src, dst_ref=dst, send_sem=ssem, recv_sem=rsem,
            device_id={"tp": lax.rem(tpi + i, TP)}, device_id_type=MESH,
        )

    for f in fetch[:4]:
        f.wait()
    prod = out_ref[...].astype(F32) * go_ref[...].astype(F32)
    high = prod.astype(BF16)
    rest = (prod - high.astype(F32)).astype(BF16)
    head_of = lax.broadcasted_iota(jnp.int32, (8 * -(-H // 8), H * VDIM), 1) // VDIM
    picks = (head_of == lax.broadcasted_iota(jnp.int32, head_of.shape, 0)).astype(F32).astype(BF16)
    deltas = dot(picks, high, ((1,), (1,))) + dot(picks, rest, ((1,), (1,)))
    logs = log_ref[...] * log2e
    for j in range(H):
        start = HEAD * j
        qs[j, :T, :] = jnp.concatenate(
            [q_ref[:, start : start + NOPE], go_ref[:, VDIM * j : VDIM * (j + 1)]], axis=1)
        turned = q_ref[:, start + NOPE : start + HEAD]
        qs[j, T : T + quarter, :] = jnp.concatenate(
            [turned[quarter * i : quarter * (i + 1)] for i in range(LANES // ROPE)], axis=1)
        terms = three_terms(logs[j : j + 1]) + three_terms(deltas[j : j + 1])
        qs[j, T + quarter :, :] = jnp.concatenate(
            [t.astype(F32) for t in terms] + [jnp.zeros((STATS - 6, T), F32)], axis=0).astype(BF16)
    wq[y, a] = qs[a]
    pl.semaphore_wait(barrier, H - 1 + GY - 1 + GX - 1 + TP - 1)

    def first_q(d):
        to = partner(H, a, d, 1)
        return copy(qs.at[to], wq.at[y, a], s1q.at[d - 1], r1q.at[d - 1], at_a(to))

    def first_k(d):
        to = partner(H, a, d, 1)
        return copy(pk.at[to], kb.at[x, a], s1k.at[d - 1], r1k.at[d - 1], at_a(to))

    def first_r(d):
        return copy(rot_ref, rk.at[x, a], s9a.at[d - 1], r9a.at[d - 1], at_a(partner(H, a, d, 1)))

    def relay_r(d, e):
        src = rk.at[x, partner(H, a, d, -1)]
        return copy(src, src, s9x.at[e - 1, d], r9x.at[e - 1, d], at_x(e))

    def over_r(d, e):
        src = rk.at[lax.rem(x + e, GX), partner(H, a, d, -1)]
        return pltpu.make_async_remote_copy(
            src_ref=src, dst_ref=src, send_sem=s9t.at[e, d], recv_sem=r9t.at[e, d],
            device_id={"tp": tpi + 1 - 2 * lax.rem(tpi, 2)}, device_id_type=MESH,
        )

    def leading(body):
        if TP % 2:
            body()
        else:
            pl.when(lax.rem(tpi, 2) == 1)(body)

    def hand_over(d, e):
        if TP % 2 == 0:
            over_r(d, e).start()

    def relay_q(d, e):
        src = wq.at[y, partner(H, a, d, -1)]
        return copy(src, src, s2q.at[e - 1, d], r2q.at[e - 1, d], at_y(e))

    def relay_k(d, e):
        src = kb.at[x, partner(H, a, d, -1)]
        return copy(src, src, s2k.at[e - 1, d], r2k.at[e - 1, d], at_x(e))

    for d in far:
        first_q(d).start()
    repeat(1, GY, lambda e: relay_q(0, e).start())
    for f in fetch[4:]:
        f.wait()
    joined = dot(lat_ref[...], w_ref[...], ((1,), (0,))).astype(BF16)
    for j in range(H):
        pk[j] = joined[:, LANES * j : LANES * (j + 1)]
    kb[x, a] = pk[a]
    rk[x, a] = rot_ref[...]
    for d in far:
        first_k(d).start()
    repeat(1, GX, lambda e: relay_k(0, e).start())

    @leading
    def _():
        for d in far:
            first_r(d).start()
        for e in range(1, GX):
            relay_r(0, e).start()

    lb[a] = lat_ref[...].reshape(lb.shape[1:])
    for d in far:
        first_q(d).wait_recv()
        repeat(1, GY, lambda e: relay_q(d, e).start())
    for d in far:
        first_k(d).wait_recv()
        repeat(1, GX, lambda e: relay_k(d, e).start())

    @leading
    def _():
        for d in far:
            first_r(d).wait_recv()
            for e in range(1, GX):
                relay_r(d, e).start()
            hand_over(d, 0)

    slab = T // TP
    mine = lat_ref.at[pl.ds(pl.multiple_of(tpi * slab, slab), slab)]

    def first_l(d):
        return copy(mine, lb.at[a, tpi], s1l.at[d - 1], r1l.at[d - 1], at_a(partner(H, a, d, 1)))

    def hand_on(d, i):
        piece = lb.at[partner(H, a, d, -1), tpi]
        return copy_tp(piece, piece, s8.at[d - 1, i - 1], r8.at[d - 1, i - 1], i)

    for d in far:
        first_l(d).start()

    def keys_of(e, units):
        where = lax.rem(x + e, GX)
        tall, wide, turned = [], [], []
        for u in units:
            kv = kb[where, u]
            rot = rk[where, u]
            lane = lax.broadcasted_iota(jnp.int32, (T, LANES), 1)
            part = jnp.where(lane < NOPE, kv, jnp.zeros_like(kv))
            column = rot.astype(F32).T.astype(BF16)
            tall.append(jnp.concatenate([part, column, jnp.zeros((T, LANES - ROPE), BF16)], axis=1))
            wide.append(kv - part)
            turned.append(jnp.concatenate([kv.astype(F32).T.astype(BF16)[:NOPE], rot], axis=0))
        return jnp.concatenate(tall, axis=0), jnp.concatenate(wide, axis=0), jnp.concatenate(turned, axis=1)

    wide = H * T
    order = [0] + far
    chunk = 2 if H % 2 == 0 else 1
    chunks = H // chunk

    def prepare(f):
        col = lax.rem(y + f, GY)
        for j in range(H):
            packed = wq[col, j, T : T + quarter, :]
            for k in range(LANES // ROPE):
                part = packed if k == 0 else jnp.concatenate(
                    [packed[:, ROPE * k :], packed[:, : ROPE * k]], axis=1)
                rp[f, T * j + quarter * k : T * j + quarter * (k + 1), :] = part

    def attend(keys, f):
        key, value, turned = keys
        col = lax.rem(y + f, GY)
        row = wq[col, :, :T, :].reshape(wide, LANES)
        both = jnp.concatenate([row, rp[f]], axis=1)
        stats = [wq[col, j, T + quarter :, :].astype(F32) for j in range(H)]
        log = jnp.concatenate([t[0:1] + t[1:2] + t[2:3] for t in stats], axis=1)
        delta = jnp.concatenate([t[3:4] + t[4:5] + t[5:6] for t in stats], axis=1)
        s = dot(key, both, ((1,), (1,)))
        dp = dot(value, row, ((1,), (1,)))
        p = jnp.exp2(s * (scale * log2e) - log)
        ds = (p * (dp - delta)).astype(BF16)
        dq = dot(turned, ds, ((1,), (0,)))
        dk = dot(ds, both, ((1,), (0,)))
        dv = dot(p.astype(BF16), row, ((1,), (0,)))
        return dq, dk, dv

    def unit_of(k, sign):
        return partner(H, a, order[k], sign)

    def span(n):
        return pl.ds(wide // chunks * n, wide // chunks)

    def keys_at(e, n):
        return keys_of(e, [unit_of(n * chunk + c, -1) for c in range(chunk)])

    def whole_keys(e):
        return keys_of(e, [unit_of(k, -1) for k in range(H)])

    def gather(e, n, dk, dv, first):
        if first:
            dka[e, span(n), :] = dk
            dva[e, span(n), :] = dv
        else:
            dka[e, span(n), :] += dk
            dva[e, span(n), :] += dv

    def gather_all(e, dk, dv, first):
        for n in range(chunks):
            part = slice(wide // chunks * n, wide // chunks * (n + 1))
            gather(e, n, dk[part], dv[part], first)

    def pair(e, n):
        dk, dv = dka[e, span(n), :LANES], dva[e, span(n), :]
        lane = lax.broadcasted_iota(jnp.int32, dv.shape, 1)
        return jnp.where(lane < NOPE, dk * scale, dv)

    def turned_part(e):
        return (dka[e, :, LANES:] * scale).T[:ROPE]

    def back_k(e, n):
        piece = pl.ds(n * chunk, chunk)
        return copy(kvs.at[e - 1, piece], kvr.at[e - 1, piece], s3k.at[e - 1, n], r3k.at[e - 1, n], at_x(e))

    def back_q(f):
        return copy(dqs.at[f - 1], dqr.at[f - 1], s3q.at[f - 1], r3q.at[f - 1], at_y(f))

    def back_r(e):
        return copy(rps.at[e - 1], rpr.at[e - 1], s9b.at[e - 1], r9b.at[e - 1], at_x(e))

    def send_k(e, n):
        kv = pair(e, n)
        for c in range(chunk):
            kvs[e - 1, n * chunk + c] = kv[T * c : T * (c + 1)].astype(KV_PART)
        back_k(e, n).start()

    def take_over(e, ds):
        if TP % 2 == 0:
            @pl.when(lax.rem(tpi, 2) == 0)
            def _():
                for d in ds:
                    over_r(d, e).wait_recv()

    def send_r():
        for e in range(1, GX):
            rps[e - 1] = turned_part(e).astype(KV_PART)
            back_r(e).start()

    take_over(0, far)
    prepare(0)
    dq, dk, dv = attend(whole_keys(0), 0)
    dqa[0] = dq
    gather_all(0, dk, dv, True)
    for e in range(1, GX):
        for d in order:
            relay_k(d, GX - e).wait_recv()

        @leading
        def _():
            for d in order:
                relay_r(d, GX - e).wait_recv()
                hand_over(d, e)

        take_over(e, order)
        dq, dk, dv = attend(whole_keys(e), 0)
        dqa[0] += dq
        gather_all(e, dk, dv, True)
    for f in range(1, GY):
        for d in order:
            relay_q(d, GY - f).wait_recv()
        prepare(f)
        for e in range(1, GX):
            for n in range(chunks):
                dq, dk, dv = attend(keys_at(e, n), f)
                if e == 1 and n == 0:
                    dqa[f] = dq
                else:
                    dqa[f] += dq
                gather(e, n, dk, dv, False)
                if f == GY - 1:
                    send_k(e, n)
        if f == GY - 1:
            send_r()
        dq, dk, dv = attend(whole_keys(0), f)
        dqs[f - 1] = (dqa[f] + dq if GX > 1 else dq).astype(DQ_PART)
        back_q(f).start()
        gather_all(0, dk, dv, False)
    if GY == 1:
        send_r()

    for d in far:
        first_l(d).wait_recv()
        repeat(1, TP, lambda i: hand_on(d, i).start())

    def home_k(d):
        to = partner(H, a, d, -1)
        return copy(kvo.at[order.index(d)], kvh.at[a], s4k.at[d - 1], r4k.at[d - 1], at_a(to))

    def home_r(d):
        to = partner(H, a, d, -1)
        return copy(ro.at[order.index(d)], rr.at[a], s4r.at[d - 1], r4r.at[d - 1], at_a(to))

    for d in far:
        repeat(1, TP, lambda i: hand_on(d, i).wait_recv())
    turned = turned_part(0)
    grads = []
    for n in range(chunks):
        for e in range(1, GX):
            back_k(e, n).wait_recv()
        kv = pair(0, n)
        lats, finals = [], []
        for c in range(chunk):
            slot = n * chunk + c
            part = kv[T * c : T * (c + 1)]
            for e in range(1, GX):
                part = part + kvr[e - 1, slot].astype(F32)
            part = part.astype(BF16)
            kvo[slot] = part
            lats.append(lb[unit_of(slot, -1)].reshape(T, lb.shape[3]))
            finals.append(part)
            if slot == 0:
                kvh[a] = part
            else:
                home_k(order[slot]).start()
        grads.append(dot(jnp.concatenate(lats, axis=0), jnp.concatenate(finals, axis=0), ((0,), (0,))))
    total = add_all(grads)
    rows = wgs.shape[1]
    wgs[...] = total.reshape(S, rows, LANES).astype(WG_PART)
    wgr[me] = wgs[me]

    spread = list(range(1, S))

    def share(i):
        to = lax.rem(me + i, S)
        return copy(wgs.at[to], wgr.at[me], s5.at[i - 1], r5.at[i - 1], to)

    for i in spread:
        share(i).start()

    for e in range(1, GX):
        back_r(e).wait_recv()
        turned = turned + rpr[e - 1].astype(F32)
    for slot in range(H):
        ro[slot] = turned[:, T * slot : T * (slot + 1)].astype(KV_PART)
    rr[a] = ro[0]
    for d in far:
        home_r(d).start()

    mine_q = dqa[0]
    for e in range(1, GY):
        back_q(e).wait_recv()
        mine_q = mine_q + dqr[e - 1].astype(F32)
    mine_q = (mine_q * scale).astype(BF16)
    for j in range(H):
        dqo[j] = mine_q[:, T * j : T * (j + 1)]

    def home_q(d):
        to = partner(H, a, d, 1)
        return copy(dqo.at[to], dqh.at[a], s4q.at[d - 1], r4q.at[d - 1], at_a(to))

    for d in far:
        home_q(d).start()
    dqh[a] = dqo[a]

    for d in far:
        home_k(d).wait_recv()
    for j in range(H):
        kg_ref[:, NOPE * j : NOPE * (j + 1)] = kvh[j, :, :NOPE]
        vg_ref[:, VDIM * j : VDIM * (j + 1)] = kvh[j, :, NOPE:]
    for d in far:
        home_r(d).wait_recv()
    rt[tpi] = add_all([rr[j].astype(F32) for j in range(H)])

    def swap(i):
        return copy_tp(rt.at[tpi], rt.at[tpi], s6.at[i - 1], r6.at[i - 1], i)

    repeat(1, TP, lambda i: swap(i).start())
    for d in far:
        home_q(d).wait_recv()
    qg_ref[...] = dqh[...].reshape(H * HEAD, T).astype(F32).T.astype(BF16)
    repeat(1, TP, lambda i: swap(i).wait_recv())
    rg_ref[...] = add_all([rt[i] for i in range(TP)])

    for i in spread:
        share(i).wait_recv()
    for j in range(H):
        wg_ref[:, LANES * j : LANES * (j + 1)] = add_all([wgr[i * H + j].astype(F32) for i in range(G)])

    for d in far:
        for c in (first_q(d), first_k(d), first_l(d), home_k(d), home_r(d), home_q(d)):
            c.wait_send()
        repeat(1, TP, lambda i: hand_on(d, i).wait_send())
    for d in order:
        repeat(1, GY, lambda e: relay_q(d, e).wait_send())
        repeat(1, GX, lambda e: relay_k(d, e).wait_send())
    for n in range(chunks):
        repeat(1, GX, lambda e: back_k(e, n).wait_send())
    repeat(1, GY, lambda e: back_q(e).wait_send())
    repeat(1, TP, lambda i: swap(i).wait_send())
    for i in spread:
        share(i).wait_send()

    @leading
    def _():
        for d in far:
            first_r(d).wait_send()
        for e in range(1, GX):
            for d in order:
                relay_r(d, e).wait_send()
        if TP % 2 == 0:
            for d in far:
                over_r(d, 0).wait_send()
            for e in range(1, GX):
                for d in order:
                    over_r(d, e).wait_send()

    for e in range(1, GX):
        back_r(e).wait_send()


def put_out(*refs):
    copies = [pltpu.make_async_copy(refs[i], refs[5 + i], refs[10].at[i]) for i in range(5)]
    for c in copies:
        c.start()
    for c in copies:
        c.wait()


def per_device(S, TP, queries, latents, rot_key, kv_weight, log_sums, outputs, out_grad):
    T, rank = latents.shape
    H = log_sums.shape[1]
    G = S // H
    GX = max(d for d in range(1, math.isqrt(G) + 1) if G % d == 0)
    GY = G // GX
    rows = rank // S
    wide = H * T
    dma = lambda *n: pltpu.SemaphoreType.DMA(tuple(max(k, 1) for k in n))
    pairs = lambda *n: [dma(*n), dma(*n)]
    vm = lambda shape, kind: pltpu.VMEM(tuple(max(k, 1) for k in shape), kind)
    unit = T + T * ROPE // LANES + STATS
    arrays = (queries, latents, rot_key.T, kv_weight, log_sums.T, outputs, out_grad)
    scratch = [
        *[vm(u.shape, u.dtype) for u in arrays], dma(len(arrays)),
        vm((H, unit, LANES), BF16), vm((H, T, LANES), BF16),
        vm((GY, H, unit, LANES), BF16), vm((GX, H, T, LANES), BF16), vm((GX, H, ROPE, T), BF16), vm((H, TP, T // TP, rank), BF16),
        vm((GY, wide, LANES), BF16), vm((GY, HEAD, wide), F32),
        *[vm((GY - 1, HEAD, wide), DQ_PART)] * 2, *[vm((GX - 1, H, T, LANES), KV_PART)] * 2, *[vm((GX - 1, ROPE, wide), KV_PART)] * 2,
        vm((GX, wide, 2 * LANES), F32), vm((GX, wide, LANES), F32),
        *[vm((H, T, LANES), BF16)] * 2, *[vm((H, ROPE, T), KV_PART)] * 2, vm((TP, ROPE, T), F32),
        *[vm((S, rows, LANES), WG_PART)] * 2, *[vm((H, HEAD, T), BF16)] * 2,
        *pairs(H - 1), *pairs(H - 1), *pairs(H - 1), *pairs(GY - 1, H), *pairs(GX - 1, H),
        *pairs(GY - 1), *pairs(GX - 1, H),
        *pairs(H - 1), *pairs(H - 1), *pairs(H - 1), *pairs(S - 1), *pairs(TP - 1), *pairs(H - 1, TP - 1),
        *pairs(H - 1), *pairs(GX - 1, H), *pairs(GX, H), *pairs(GX - 1),
    ]
    shapes = [
        ((T, H * HEAD), BF16), ((T, H * NOPE), BF16), ((T, H * VDIM), BF16),
        ((ROPE, T), F32), ((rows, H * LANES), F32),
    ]
    held = sum(u[0] * -(-u[1] // LANES) * LANES * jnp.dtype(t).itemsize for u, t in shapes)
    results = pl.pallas_call(
        functools.partial(kernel, S, TP, H, GY, GX),
        out_shape=[pltpu.VMEM(*u) for u in shapes],
        in_specs=[pl.BlockSpec(memory_space=pltpu.HBM)] * 7,
        out_specs=[pl.BlockSpec(memory_space=pltpu.VMEM)] * 5,
        scratch_shapes=scratch,
        compiler_params=pltpu.CompilerParams(
            collective_id=0, has_side_effects=True, vmem_limit_bytes=VMEM_BYTES - held - SPARE
        ),
    )(*arrays)
    query_grad, key_grad, value_grad, rot_grad, weight_grad = pl.pallas_call(
        put_out,
        out_shape=[jax.ShapeDtypeStruct(*u) for u in shapes],
        in_specs=[pl.BlockSpec(memory_space=pltpu.VMEM)] * 5,
        out_specs=[pl.BlockSpec(memory_space=pltpu.HBM)] * 5,
        scratch_shapes=[dma(5)],
        compiler_params=pltpu.CompilerParams(vmem_limit_bytes=1 << 20),
    )(*results)
    return query_grad, key_grad, value_grad, rot_grad.T, weight_grad


def solution(mesh):
    placed = (
        P("sp", "tp"), P("sp", None), P("sp", None), P(None, "tp"),
        P("sp", "tp"), P("sp", "tp"), P("sp", "tp"),
    )
    return jax.shard_map(
        functools.partial(per_device, mesh.shape["sp"], mesh.shape["tp"]),
        mesh=mesh,
        in_specs=placed,
        out_specs=(P("sp", "tp"), P("sp", "tp"), P("sp", "tp"), P("sp", None), P("sp", "tp")),
        check_vma=False,
    )
```

```python
import functools
import math

import jax
import jax.numpy as jnp
from jax import lax
from jax.experimental import pallas as pl
from jax.experimental.pallas import tpu as pltpu
from jax.sharding import PartitionSpec as P

NOPE = 64
ROPE = 32
VDIM = 64
HEAD = NOPE + ROPE
LANES = 128
STATS = 8
VMEM_BYTES = 67043328
SPARE = 8192
MESH = pl.DeviceIdType.MESH
F32 = jnp.float32
BF16 = jnp.bfloat16
KV_PART = BF16
DQ_PART = BF16
WG_PART = BF16


def dot(x, y, dims):
    return lax.dot_general(x, y, (dims, ((), ())), preferred_element_type=F32)


def three_terms(x):
    hi = x.astype(BF16)
    rest = x - hi.astype(F32)
    mid = rest.astype(BF16)
    low = (rest - mid.astype(F32)).astype(BF16)
    return hi, mid, low


def repeat(start, stop, body):
    if stop - start <= 4:
        for i in range(start, stop):
            body(i)
    else:
        def step(i, carry):
            body(i)
            return carry

        lax.fori_loop(start, stop, step, 0)


def add_all(terms):
    return functools.reduce(lambda x, y: x + y, terms)


def power_of_two(n):
    return n & (n - 1) == 0


def partner(n, i, d, sign):
    if not power_of_two(n):
        return lax.rem(i + sign * d + n, n)
    bit = 1
    result = i
    while bit <= d:
        if d & bit:
            result = result + bit * (1 - 2 * lax.rem(i // bit, 2))
        bit *= 2
    return result


def distances(n):
    if not power_of_two(n):
        return list(range(1, n))
    return sorted(range(1, n), key=lambda d: -bin(d).count("1"))


def kernel(
    S, TP, H, GY, GX,
    q_in, lat_in, rot_in, w_in, log_in, out_in, go_in,
    qg_ref, kg_ref, vg_ref, rg_ref, wg_ref,
    q_ref, lat_ref, rot_ref, w_ref, log_ref, out_ref, go_ref, loads,
    qs, pk, wq, kb, rk, lb, rp, dqa, dqs, dqr, kvs, kvr, rps, rpr, dka, dva,
    kvo, kvh, ro, rr, rt, wgs, wgr, dqo, dqh,
    s1q, r1q, s1k, r1k, s1l, r1l, s2q, r2q, s2k, r2k, s3q, r3q, s3k, r3k,
    s4q, r4q, s4k, r4k, s4r, r4r, s5, r5, s6, r6, s8, r8,
    s9a, r9a, s9x, r9x, s9t, r9t, s9b, r9b,
):
    G = GY * GX
    T = q_ref.shape[0]
    me = lax.axis_index("sp")
    tpi = lax.axis_index("tp")
    a, b = lax.rem(me, H), me // H
    y, x = b // GX, lax.rem(b, GX)
    scale = HEAD ** (-0.5)
    log2e = math.log2(math.e)
    far = distances(H)
    quarter = T * ROPE // LANES

    barrier = pltpu.get_barrier_semaphore()

    def greet(to):
        pl.semaphore_signal(barrier, inc=1, device_id={"sp": to}, device_id_type=MESH)

    def greet_tp(i):
        pl.semaphore_signal(barrier, inc=1, device_id={"tp": lax.rem(tpi + i, TP)}, device_id_type=MESH)

    def at_a(z):
        return b * H + z

    def at_y(e):
        return (lax.rem(y + e, GY) * GX + x) * H + a

    def at_x(e):
        return (y * GX + lax.rem(x + e, GX)) * H + a

    pairs = (
        (q_in, q_ref), (go_in, go_ref), (out_in, out_ref), (log_in, log_ref),
        (lat_in, lat_ref), (w_in, w_ref), (rot_in, rot_ref),
    )
    fetch = [pltpu.make_async_copy(u, v, loads.at[i]) for i, (u, v) in enumerate(pairs)]
    for f in fetch:
        f.start()
    for d in far:
        greet(at_a(partner(H, a, d, 1)))
    repeat(1, GY, lambda e: greet(at_y(e)))
    repeat(1, GX, lambda e: greet(at_x(e)))
    repeat(1, TP, greet_tp)

    def copy(src, dst, ssem, rsem, sp):
        return pltpu.make_async_remote_copy(
            src_ref=src, dst_ref=dst, send_sem=ssem, recv_sem=rsem,
            device_id={"sp": sp}, device_id_type=MESH,
        )

    def copy_tp(src, dst, ssem, rsem, i):
        return pltpu.make_async_remote_copy(
            src_ref=src, dst_ref=dst, send_sem=ssem, recv_sem=rsem,
            device_id={"tp": lax.rem(tpi + i, TP)}, device_id_type=MESH,
        )

    for f in fetch[:4]:
        f.wait()
    prod = out_ref[...].astype(F32) * go_ref[...].astype(F32)
    high = prod.astype(BF16)
    rest = (prod - high.astype(F32)).astype(BF16)
    head_of = lax.broadcasted_iota(jnp.int32, (8 * -(-H // 8), H * VDIM), 1) // VDIM
    picks = (head_of == lax.broadcasted_iota(jnp.int32, head_of.shape, 0)).astype(F32).astype(BF16)
    deltas = dot(picks, high, ((1,), (1,))) + dot(picks, rest, ((1,), (1,)))
    logs = log_ref[...] * log2e
    for j in range(H):
        start = HEAD * j
        qs[j, :T, :] = jnp.concatenate(
            [q_ref[:, start : start + NOPE], go_ref[:, VDIM * j : VDIM * (j + 1)]], axis=1)
        turned = q_ref[:, start + NOPE : start + HEAD]
        qs[j, T : T + quarter, :] = jnp.concatenate(
            [turned[quarter * i : quarter * (i + 1)] for i in range(LANES // ROPE)], axis=1)
        terms = three_terms(logs[j : j + 1]) + three_terms(deltas[j : j + 1])
        qs[j, T + quarter :, :] = jnp.concatenate(
            [t.astype(F32) for t in terms] + [jnp.zeros((STATS - 6, T), F32)], axis=0).astype(BF16)
    wq[y, a] = qs[a]
    pl.semaphore_wait(barrier, H - 1 + GY - 1 + GX - 1 + TP - 1)

    def first_q(d):
        to = partner(H, a, d, 1)
        return copy(qs.at[to], wq.at[y, a], s1q.at[d - 1], r1q.at[d - 1], at_a(to))

    def first_k(d):
        to = partner(H, a, d, 1)
        return copy(pk.at[to], kb.at[x, a], s1k.at[d - 1], r1k.at[d - 1], at_a(to))

    def first_r(d):
        return copy(rot_ref, rk.at[x, a], s9a.at[d - 1], r9a.at[d - 1], at_a(partner(H, a, d, 1)))

    def relay_r(d, e):
        src = rk.at[x, partner(H, a, d, -1)]
        return copy(src, src, s9x.at[e - 1, d], r9x.at[e - 1, d], at_x(e))

    def over_r(d, e):
        src = rk.at[lax.rem(x + e, GX), partner(H, a, d, -1)]
        return pltpu.make_async_remote_copy(
            src_ref=src, dst_ref=src, send_sem=s9t.at[e, d], recv_sem=r9t.at[e, d],
            device_id={"tp": tpi + 1 - 2 * lax.rem(tpi, 2)}, device_id_type=MESH,
        )

    def leading(body):
        if TP % 2:
            body()
        else:
            pl.when(lax.rem(tpi, 2) == 1)(body)

    def hand_over(d, e):
        if TP % 2 == 0:
            over_r(d, e).start()

    def relay_q(d, e):
        src = wq.at[y, partner(H, a, d, -1)]
        return copy(src, src, s2q.at[e - 1, d], r2q.at[e - 1, d], at_y(e))

    def relay_k(d, e):
        src = kb.at[x, partner(H, a, d, -1)]
        return copy(src, src, s2k.at[e - 1, d], r2k.at[e - 1, d], at_x(e))

    for d in far:
        first_q(d).start()
    repeat(1, GY, lambda e: relay_q(0, e).start())
    for f in fetch[4:]:
        f.wait()
    joined = dot(lat_ref[...], w_ref[...], ((1,), (0,))).astype(BF16)
    for j in range(H):
        pk[j] = joined[:, LANES * j : LANES * (j + 1)]
    kb[x, a] = pk[a]
    rk[x, a] = rot_ref[...]
    for d in far:
        first_k(d).start()
    repeat(1, GX, lambda e: relay_k(0, e).start())

    @leading
    def _():
        for d in far:
            first_r(d).start()
        for e in range(1, GX):
            relay_r(0, e).start()

    lb[a] = lat_ref[...].reshape(lb.shape[1:])
    for d in far:
        first_q(d).wait_recv()
        repeat(1, GY, lambda e: relay_q(d, e).start())
    for d in far:
        first_k(d).wait_recv()
        repeat(1, GX, lambda e: relay_k(d, e).start())

    @leading
    def _():
        for d in far:
            first_r(d).wait_recv()
            for e in range(1, GX):
                relay_r(d, e).start()
            hand_over(d, 0)

    slab = T // TP
    mine = lat_ref.at[pl.ds(pl.multiple_of(tpi * slab, slab), slab)]

    def first_l(d):
        return copy(mine, lb.at[a, tpi], s1l.at[d - 1], r1l.at[d - 1], at_a(partner(H, a, d, 1)))

    def hand_on(d, i):
        piece = lb.at[partner(H, a, d, -1), tpi]
        return copy_tp(piece, piece, s8.at[d - 1, i - 1], r8.at[d - 1, i - 1], i)

    def keys_of(e, units):
        where = lax.rem(x + e, GX)
        tall, wide, turned = [], [], []
        for u in units:
            kv = kb[where, u]
            rot = rk[where, u]
            lane = lax.broadcasted_iota(jnp.int32, (T, LANES), 1)
            part = jnp.where(lane < NOPE, kv, jnp.zeros_like(kv))
            column = rot.astype(F32).T.astype(BF16)
            tall.append(jnp.concatenate([part, column, jnp.zeros((T, LANES - ROPE), BF16)], axis=1))
            wide.append(kv - part)
            turned.append(jnp.concatenate([kv.astype(F32).T.astype(BF16)[:NOPE], rot], axis=0))
        return jnp.concatenate(tall, axis=0), jnp.concatenate(wide, axis=0), jnp.concatenate(turned, axis=1)

    wide = H * T
    order = [0] + far
    chunk = 2 if H % 2 == 0 else 1
    chunks = H // chunk

    def prepare(f):
        col = lax.rem(y + f, GY)
        for j in range(H):
            packed = wq[col, j, T : T + quarter, :]
            for k in range(LANES // ROPE):
                part = packed if k == 0 else jnp.concatenate(
                    [packed[:, ROPE * k :], packed[:, : ROPE * k]], axis=1)
                rp[f, T * j + quarter * k : T * j + quarter * (k + 1), :] = part

    def attend(keys, f):
        key, value, turned = keys
        col = lax.rem(y + f, GY)
        row = wq[col, :, :T, :].reshape(wide, LANES)
        both = jnp.concatenate([row, rp[f]], axis=1)
        stats = [wq[col, j, T + quarter :, :].astype(F32) for j in range(H)]
        log = jnp.concatenate([t[0:1] + t[1:2] + t[2:3] for t in stats], axis=1)
        delta = jnp.concatenate([t[3:4] + t[4:5] + t[5:6] for t in stats], axis=1)
        s = dot(key, both, ((1,), (1,)))
        dp = dot(value, row, ((1,), (1,)))
        p = jnp.exp2(s * (scale * log2e) - log)
        ds = (p * (dp - delta)).astype(BF16)
        dq = dot(turned, ds, ((1,), (0,)))
        dk = dot(ds, both, ((1,), (0,)))
        dv = dot(p.astype(BF16), row, ((1,), (0,)))
        return dq, dk, dv

    def unit_of(k, sign):
        return partner(H, a, order[k], sign)

    def span(n):
        return pl.ds(wide // chunks * n, wide // chunks)

    def keys_at(e, n):
        return keys_of(e, [unit_of(n * chunk + c, -1) for c in range(chunk)])

    def whole_keys(e):
        return keys_of(e, [unit_of(k, -1) for k in range(H)])

    def gather(e, n, dk, dv, first):
        if first:
            dka[e, span(n), :] = dk
            dva[e, span(n), :] = dv
        else:
            dka[e, span(n), :] += dk
            dva[e, span(n), :] += dv

    def gather_all(e, dk, dv, first):
        for n in range(chunks):
            part = slice(wide // chunks * n, wide // chunks * (n + 1))
            gather(e, n, dk[part], dv[part], first)

    def pair(e, n):
        dk, dv = dka[e, span(n), :LANES], dva[e, span(n), :]
        lane = lax.broadcasted_iota(jnp.int32, dv.shape, 1)
        return jnp.where(lane < NOPE, dk * scale, dv)

    def turned_part(e):
        return (dka[e, :, LANES:] * scale).T[:ROPE]

    def back_k(e, n):
        piece = pl.ds(n * chunk, chunk)
        return copy(kvs.at[e - 1, piece], kvr.at[e - 1, piece], s3k.at[e - 1, n], r3k.at[e - 1, n], at_x(e))

    def back_q(f):
        return copy(dqs.at[f - 1], dqr.at[f - 1], s3q.at[f - 1], r3q.at[f - 1], at_y(f))

    def back_r(e):
        return copy(rps.at[e - 1], rpr.at[e - 1], s9b.at[e - 1], r9b.at[e - 1], at_x(e))

    def send_k(e, n):
        kv = pair(e, n)
        for c in range(chunk):
            kvs[e - 1, n * chunk + c] = kv[T * c : T * (c + 1)].astype(KV_PART)
        back_k(e, n).start()

    def take_over(e, ds):
        if TP % 2 == 0:
            @pl.when(lax.rem(tpi, 2) == 0)
            def _():
                for d in ds:
                    over_r(d, e).wait_recv()

    def send_r():
        for e in range(1, GX):
            rps[e - 1] = turned_part(e).astype(KV_PART)
            back_r(e).start()

    take_over(0, far)
    prepare(0)
    dq, dk, dv = attend(whole_keys(0), 0)
    dqa[0] = dq
    gather_all(0, dk, dv, True)
    for d in far:
        first_l(d).start()
    for e in range(1, GX):
        for d in order:
            relay_k(d, GX - e).wait_recv()

        @leading
        def _():
            for d in order:
                relay_r(d, GX - e).wait_recv()
                hand_over(d, e)

        take_over(e, order)
        dq, dk, dv = attend(whole_keys(e), 0)
        dqa[0] += dq
        gather_all(e, dk, dv, True)
    for f in range(1, GY):
        for d in order:
            relay_q(d, GY - f).wait_recv()
        prepare(f)
        for e in range(1, GX):
            for n in range(chunks):
                dq, dk, dv = attend(keys_at(e, n), f)
                if e == 1 and n == 0:
                    dqa[f] = dq
                else:
                    dqa[f] += dq
                gather(e, n, dk, dv, False)
                if f == GY - 1:
                    send_k(e, n)
        if f == GY - 1:
            send_r()
        dq, dk, dv = attend(whole_keys(0), f)
        dqs[f - 1] = (dqa[f] + dq if GX > 1 else dq).astype(DQ_PART)
        back_q(f).start()
        gather_all(0, dk, dv, False)
    if GY == 1:
        send_r()

    for d in far:
        first_l(d).wait_recv()
        repeat(1, TP, lambda i: hand_on(d, i).start())

    def home_k(d):
        to = partner(H, a, d, -1)
        return copy(kvo.at[order.index(d)], kvh.at[a], s4k.at[d - 1], r4k.at[d - 1], at_a(to))

    def home_r(d):
        to = partner(H, a, d, -1)
        return copy(ro.at[order.index(d)], rr.at[a], s4r.at[d - 1], r4r.at[d - 1], at_a(to))

    for d in far:
        repeat(1, TP, lambda i: hand_on(d, i).wait_recv())
    turned = turned_part(0)
    grads = []
    for n in range(chunks):
        for e in range(1, GX):
            back_k(e, n).wait_recv()
        kv = pair(0, n)
        lats, finals = [], []
        for c in range(chunk):
            slot = n * chunk + c
            part = kv[T * c : T * (c + 1)]
            for e in range(1, GX):
                part = part + kvr[e - 1, slot].astype(F32)
            part = part.astype(BF16)
            kvo[slot] = part
            lats.append(lb[unit_of(slot, -1)].reshape(T, lb.shape[3]))
            finals.append(part)
            if slot == 0:
                kvh[a] = part
            else:
                home_k(order[slot]).start()
        grads.append(dot(jnp.concatenate(lats, axis=0), jnp.concatenate(finals, axis=0), ((0,), (0,))))
    total = add_all(grads)
    rows = wgs.shape[1]
    wgs[...] = total.reshape(S, rows, LANES).astype(WG_PART)
    wgr[me] = wgs[me]

    spread = list(range(1, S))

    def share(i):
        to = lax.rem(me + i, S)
        return copy(wgs.at[to], wgr.at[me], s5.at[i - 1], r5.at[i - 1], to)

    def send_shares():
        for i in spread:
            share(i).start()

    pl.when(lax.rem(tpi, 2) == 0)(send_shares)

    for e in range(1, GX):
        back_r(e).wait_recv()
        turned = turned + rpr[e - 1].astype(F32)
    for slot in range(H):
        ro[slot] = turned[:, T * slot : T * (slot + 1)].astype(KV_PART)
    rr[a] = ro[0]
    for d in far:
        home_r(d).start()

    mine_q = dqa[0]
    for e in range(1, GY):
        back_q(e).wait_recv()
        mine_q = mine_q + dqr[e - 1].astype(F32)
    mine_q = (mine_q * scale).astype(BF16)
    for j in range(H):
        dqo[j] = mine_q[:, T * j : T * (j + 1)]

    def home_q(d):
        to = partner(H, a, d, 1)
        return copy(dqo.at[to], dqh.at[a], s4q.at[d - 1], r4q.at[d - 1], at_a(to))

    for d in far:
        home_q(d).start()
    pl.when(lax.rem(tpi, 2) == 1)(send_shares)
    dqh[a] = dqo[a]

    for d in far:
        home_k(d).wait_recv()
    for j in range(H):
        kg_ref[:, NOPE * j : NOPE * (j + 1)] = kvh[j, :, :NOPE]
        vg_ref[:, VDIM * j : VDIM * (j + 1)] = kvh[j, :, NOPE:]
    for d in far:
        home_r(d).wait_recv()
    rt[tpi] = add_all([rr[j].astype(F32) for j in range(H)])

    def swap(i):
        return copy_tp(rt.at[tpi], rt.at[tpi], s6.at[i - 1], r6.at[i - 1], i)

    repeat(1, TP, lambda i: swap(i).start())
    for d in far:
        home_q(d).wait_recv()
    qg_ref[...] = dqh[...].reshape(H * HEAD, T).astype(F32).T.astype(BF16)
    repeat(1, TP, lambda i: swap(i).wait_recv())
    rg_ref[...] = add_all([rt[i] for i in range(TP)])

    for i in spread:
        share(i).wait_recv()
    for j in range(H):
        wg_ref[:, LANES * j : LANES * (j + 1)] = add_all([wgr[i * H + j].astype(F32) for i in range(G)])

    for d in far:
        for c in (first_q(d), first_k(d), first_l(d), home_k(d), home_r(d), home_q(d)):
            c.wait_send()
        repeat(1, TP, lambda i: hand_on(d, i).wait_send())
    for d in order:
        repeat(1, GY, lambda e: relay_q(d, e).wait_send())
        repeat(1, GX, lambda e: relay_k(d, e).wait_send())
    for n in range(chunks):
        repeat(1, GX, lambda e: back_k(e, n).wait_send())
    repeat(1, GY, lambda e: back_q(e).wait_send())
    repeat(1, TP, lambda i: swap(i).wait_send())
    for i in spread:
        share(i).wait_send()

    @leading
    def _():
        for d in far:
            first_r(d).wait_send()
        for e in range(1, GX):
            for d in order:
                relay_r(d, e).wait_send()
        if TP % 2 == 0:
            for d in far:
                over_r(d, 0).wait_send()
            for e in range(1, GX):
                for d in order:
                    over_r(d, e).wait_send()

    for e in range(1, GX):
        back_r(e).wait_send()


def put_out(*refs):
    copies = [pltpu.make_async_copy(refs[i], refs[5 + i], refs[10].at[i]) for i in range(5)]
    for c in copies:
        c.start()
    for c in copies:
        c.wait()


def per_device(S, TP, queries, latents, rot_key, kv_weight, log_sums, outputs, out_grad):
    T, rank = latents.shape
    H = log_sums.shape[1]
    G = S // H
    GX = max(d for d in range(1, math.isqrt(G) + 1) if G % d == 0)
    GY = G // GX
    rows = rank // S
    wide = H * T
    dma = lambda *n: pltpu.SemaphoreType.DMA(tuple(max(k, 1) for k in n))
    pairs = lambda *n: [dma(*n), dma(*n)]
    vm = lambda shape, kind: pltpu.VMEM(tuple(max(k, 1) for k in shape), kind)
    unit = T + T * ROPE // LANES + STATS
    arrays = (queries, latents, rot_key.T, kv_weight, log_sums.T, outputs, out_grad)
    scratch = [
        *[vm(u.shape, u.dtype) for u in arrays], dma(len(arrays)),
        vm((H, unit, LANES), BF16), vm((H, T, LANES), BF16),
        vm((GY, H, unit, LANES), BF16), vm((GX, H, T, LANES), BF16), vm((GX, H, ROPE, T), BF16), vm((H, TP, T // TP, rank), BF16),
        vm((GY, wide, LANES), BF16), vm((GY, HEAD, wide), F32),
        *[vm((GY - 1, HEAD, wide), DQ_PART)] * 2, *[vm((GX - 1, H, T, LANES), KV_PART)] * 2, *[vm((GX - 1, ROPE, wide), KV_PART)] * 2,
        vm((GX, wide, 2 * LANES), F32), vm((GX, wide, LANES), F32),
        *[vm((H, T, LANES), BF16)] * 2, *[vm((H, ROPE, T), KV_PART)] * 2, vm((TP, ROPE, T), F32),
        *[vm((S, rows, LANES), WG_PART)] * 2, *[vm((H, HEAD, T), BF16)] * 2,
        *pairs(H - 1), *pairs(H - 1), *pairs(H - 1), *pairs(GY - 1, H), *pairs(GX - 1, H),
        *pairs(GY - 1), *pairs(GX - 1, H),
        *pairs(H - 1), *pairs(H - 1), *pairs(H - 1), *pairs(S - 1), *pairs(TP - 1), *pairs(H - 1, TP - 1),
        *pairs(H - 1), *pairs(GX - 1, H), *pairs(GX, H), *pairs(GX - 1),
    ]
    shapes = [
        ((T, H * HEAD), BF16), ((T, H * NOPE), BF16), ((T, H * VDIM), BF16),
        ((ROPE, T), F32), ((rows, H * LANES), F32),
    ]
    held = sum(u[0] * -(-u[1] // LANES) * LANES * jnp.dtype(t).itemsize for u, t in shapes)
    results = pl.pallas_call(
        functools.partial(kernel, S, TP, H, GY, GX),
        out_shape=[pltpu.VMEM(*u) for u in shapes],
        in_specs=[pl.BlockSpec(memory_space=pltpu.HBM)] * 7,
        out_specs=[pl.BlockSpec(memory_space=pltpu.VMEM)] * 5,
        scratch_shapes=scratch,
        compiler_params=pltpu.CompilerParams(
            collective_id=0, has_side_effects=True, vmem_limit_bytes=VMEM_BYTES - held - SPARE
        ),
    )(*arrays)
    query_grad, key_grad, value_grad, rot_grad, weight_grad = pl.pallas_call(
        put_out,
        out_shape=[jax.ShapeDtypeStruct(*u) for u in shapes],
        in_specs=[pl.BlockSpec(memory_space=pltpu.VMEM)] * 5,
        out_specs=[pl.BlockSpec(memory_space=pltpu.HBM)] * 5,
        scratch_shapes=[dma(5)],
        compiler_params=pltpu.CompilerParams(vmem_limit_bytes=1 << 20),
    )(*results)
    return query_grad, key_grad, value_grad, rot_grad.T, weight_grad


def solution(mesh):
    placed = (
        P("sp", "tp"), P("sp", None), P("sp", None), P(None, "tp"),
        P("sp", "tp"), P("sp", "tp"), P("sp", "tp"),
    )
    return jax.shard_map(
        functools.partial(per_device, mesh.shape["sp"], mesh.shape["tp"]),
        mesh=mesh,
        in_specs=placed,
        out_specs=(P("sp", "tp"), P("sp", "tp"), P("sp", "tp"), P("sp", None), P("sp", "tp")),
        check_vma=False,
    )
```
